32 devices in a mesh: sp: 16 (over z, y, x), tp: 2 (over core).
Axes of the slice: x: 2, y: 2, z: 4, core: 2. Of those that a mesh axis runs over, the one named last changes fastest.
Arguments:
- conv_value: bfloat16 [8192, 1536], P('sp', 'tp'), may hold values from -6 to 6
- conv_gate: bfloat16 [8192, 1536], P('sp', 'tp'), may hold values from -8 to 8
- conv_out: bfloat16 [8192, 1536], P('sp', 'tp'), may hold values from -40 to 40
- conv_taps: bfloat16 [31, 1536], P(None, 'tp'), may hold values from -1 to 1
- norm_gain: float32 [1536], P('tp'), may hold values from 0.1 to 1.9
- norm_shift: float32 [1536], P('tp'), may hold values from -3 to 3
- proj_weight: bfloat16 [2048, 1536], P(None, 'tp'), may hold values from -0.15625 to 0.15625
- out_grad: bfloat16 [8192, 2048], P('sp'), may hold values from -6 to 6
Outputs:
- grad_value: bfloat16 [8192, 1536], P('sp', 'tp')
- grad_gate: bfloat16 [8192, 1536], P('sp', 'tp')
- grad_taps: float32 [31, 1536], P(None, 'tp')
- grad_gain: float32 [1536], P('tp')
- grad_shift: float32 [1536], P('tp')
- grad_proj: float32 [2048, 1536], P('sp', 'tp')
The draws below stay inside these ranges and needn't reach their ends.
All inputs are finite; a program needn't handle non-finite values.
Results may differ from the reference program's by a relative error of at most 0.005.
Values may be sent and summed in bfloat16 or wider, within the bound.
A program may use at most 64 MiB of HBM per device.

```python
import jax
import jax.numpy as jnp
from jax import lax

D = 2048
CH = 1536
TAPS = 31
SEQ = 8192


def draw_conv_out(key, part):
    key_scale, key_group, key_base, key_mean = jax.random.split(key, 4)
    chan_scale = jnp.exp(jax.random.uniform(key_scale, (CH,), jnp.float32, -1.0, 1.0))
    group_scale = jnp.exp(jax.random.uniform(key_group, (8,), jnp.float32, -1.2, 1.2))
    group_index = jnp.arange(CH) * 8 // CH
    scales = chan_scale * group_scale[group_index]
    base = jax.random.normal(key_base, (SEQ, CH), jnp.float32) * scales
    offset = jax.random.normal(key_mean, (SEQ, 1), jnp.float32)
    return jnp.clip(base + offset, -40.0, 40.0).astype(jnp.bfloat16)


def spiked(values, rng, source, target, parts, factor):
    def block_of(position):
        return (jnp.arange(values.shape[position]) // (values.shape[position] // parts)).reshape((-1,) + (1,) * (values.ndim - 1 - position))

    one_side = jax.random.permutation(rng, parts)[block_of(target)]
    other_side = (block_of(target) + parts // 2) % parts
    return jnp.where((block_of(source) == one_side) | (block_of(source) == other_side), factor * values, values)


def steps_of(stream_key, extent, shards, smallest, high):
    def one(axis_at, parts):
        steps = jax.random.uniform(jax.random.fold_in(jax.random.fold_in(stream_key, 6), axis_at), (parts,), jnp.float32, smallest / len(shards), high / len(shards))
        return jnp.repeat(jnp.exp(steps), extent[axis_at] // parts).reshape((-1,) + (1,) * (len(extent) - axis_at - 1))

    factor_of = one(*shards[0])
    for cut in shards[1:]:
        factor_of = factor_of * one(*cut)
    return factor_of


def bell_draw(own_key, dims, scale, limit, cuts=(), held_as=jnp.bfloat16):
    entries = jax.random.normal(own_key, dims, jnp.float32) * scale
    if len(cuts) > 0:
        entries = steps_of(own_key, dims, cuts, -0.22, 0.18) * entries
    return jnp.clip(entries, min=-limit, max=limit).astype(held_as)


def noise_with(key, extent, spread, reach, pieces, heavy, held_as=jnp.bfloat16):
    drawn = spread * jax.random.normal(key, extent, jnp.float32)
    if pieces:
        drawn = drawn * steps_of(key, extent, pieces, -0.22, 0.18)
    return jnp.clip(spiked(drawn, jax.random.fold_in(key, 3), *heavy), -reach, reach).astype(held_as)


def setup_inputs(seed: int = 0) -> dict:
    splits = jax.random.split(jax.random.key(seed), 9)
    return {
        "conv_value": bell_draw(splits[0], (SEQ, CH), 1.0, 6.0, ((0, 16), (1, 2))),
        "conv_gate": bell_draw(splits[1], (SEQ, CH), 1.5, 8.0, ((0, 16), (1, 2))),
        "conv_out": draw_conv_out(jax.random.fold_in(splits[8], 71), 0),
        "conv_taps": bell_draw(splits[3], (TAPS, CH), TAPS ** -0.5, 1.0, ((1, 2),)),
        "norm_gain": jnp.clip(1.0 + 0.18 * jax.random.normal(splits[4], (CH,), jnp.float32), 0.1, 1.9),
        "norm_shift": bell_draw(splits[5], (CH,), 0.5, 3.0, ((0, 2),), jnp.float32),
        "proj_weight": bell_draw(splits[6], (D, CH), CH ** -0.5, 0.15625, ((1, 2),)),
        "out_grad": noise_with(splits[7], (SEQ, D), 1.0, 6.0, ((0, 16),), (0, 1, 16, 2.0)),
    }


norm_eps = 1e-05

def reference(conv_value, conv_gate, conv_out, conv_taps, norm_gain, norm_shift, proj_weight, out_grad):
    height = conv_out.astype(jnp.float32)
    center = lax.optimization_barrier(jnp.mean(height, axis=1, keepdims=True))
    centered = height - center
    variance = lax.optimization_barrier(jnp.mean(centered * centered, axis=1, keepdims=True))
    inv_std = lax.rsqrt(variance + norm_eps)
    normed = centered * inv_std
    shifted = normed * norm_gain + norm_shift
    sig_norm = jax.nn.sigmoid(shifted)
    active = (shifted * sig_norm).astype(jnp.bfloat16)
    grad_proj = jnp.dot(out_grad.T, active, preferred_element_type=jnp.float32)
    act_grad = jnp.dot(out_grad, proj_weight, preferred_element_type=jnp.float32)
    norm_grad = act_grad * (sig_norm * (1.0 + shifted * (1.0 - sig_norm)))
    grad_gain = lax.optimization_barrier(jnp.sum(norm_grad * normed, axis=0))
    grad_shift = lax.optimization_barrier(jnp.sum(norm_grad, axis=0))
    scaled = norm_grad * norm_gain
    height_grad = inv_std * (scaled - lax.optimization_barrier(jnp.mean(scaled, axis=1, keepdims=True)) - normed * lax.optimization_barrier(jnp.mean(scaled * normed, axis=1, keepdims=True)))
    sig_gate = jax.nn.sigmoid(conv_gate.astype(jnp.float32))
    value_float = conv_value.astype(jnp.float32)
    gated_rows = lax.optimization_barrier((value_float * sig_gate).astype(jnp.bfloat16)).astype(jnp.float32)
    tap_reach = TAPS - 1
    padded_rows = jnp.pad(gated_rows, ((tap_reach, 0), (0, 0)))
    padded_grad = jnp.pad(height_grad, ((0, tap_reach), (0, 0)))
    tap_values = conv_taps.astype(jnp.float32)
    tap_list = []
    gated_grad = jnp.zeros_like(height_grad)
    for tap_index in range(TAPS):
        tap_list.append(lax.optimization_barrier(jnp.sum(height_grad * padded_rows[tap_index:tap_index + SEQ], axis=0)))
        begin = tap_reach - tap_index
        gated_grad = gated_grad + tap_values[tap_index] * padded_grad[begin:begin + SEQ]
    grad_taps = jnp.stack(tap_list)
    grad_value = (gated_grad * sig_gate).astype(jnp.bfloat16)
    grad_gate = (gated_grad * value_float * sig_gate * (1.0 - sig_gate)).astype(jnp.bfloat16)
    return (grad_value, grad_gate, grad_taps, grad_gain, grad_shift, grad_proj)
```

```python
import functools

import jax
import jax.numpy as jnp
from jax import lax
from jax.experimental import pallas as pl
from jax.experimental.pallas import tpu as pltpu
from jax.sharding import PartitionSpec as P

norm_eps = 1e-05
MESH = pl.DeviceIdType.MESH
F32 = jnp.float32
BF16 = jnp.bfloat16
LANES = 128


def repeat(start, stop, body, unroll):
    assert (stop - start) % unroll == 0

    def step(i, carry):
        for u in range(unroll):
            body(start + i * unroll + u, carry)
        return carry

    lax.fori_loop(0, (stop - start) // unroll, step, 0)


def bit(x, b):
    return lax.rem(x // (1 << b), 2)


def coordinate_bits(index, nbits):
    bits = [bit(index, b) for b in range(nbits)]
    if nbits >= 2:
        bits[nbits - 2] = lax.rem(bits[nbits - 2] + bits[nbits - 1], 2)
    return bits


def partner_of(me, b, nbits):
    def flip(x, c):
        return x + (1 << c) * (1 - 2 * bit(me, c))

    other = flip(me, b)
    if nbits >= 2 and b == nbits - 1:
        other = flip(other, b - 1)
    return other


def stage_orders(nbits, groups):
    body = list(range(max(nbits - 1, 1)))
    tail = list(range(len(body), nbits))
    return [body[g % len(body):] + body[: g % len(body)] + tail for g in range(groups)]


def kernel(
    dims,
    cv_hbm, cg_hbm, co_hbm, taps_ref, gain_ref, shift_ref, w_hbm, og_hbm,
    gv, gg, taps_out, gain_out, shift_out, proj_out,
    cv, cg, co, w, og, ogt, active, normed, dsilu, scaled, hgx,
    st_a, st_b, st_d, pk_a, pk_b, pk_c, pk_d, tapf, acc, sendbuf, recvbuf, tapacc, rowacc, flat, parts, mine, whole,
    in_sem, tp_send, tp_recv, halo_send, halo_recv,
    rs_send, rs_recv, a_send, a_recv, b_send, b_recv,
):
    n, nbits, groups, chan_total = dims
    rows, chan = co.shape
    width = og.shape[1]
    block = width // n
    gcols = chan // groups
    cblocks = chan // LANES
    ntaps = taps_ref.shape[0]
    reach = ntaps - 1
    halo = hgx.shape[1] - rows
    chunk = mine.shape[0]
    per = -(-(ntaps + 2) // 8) * 8
    me = lax.axis_index("sp")
    core = lax.axis_index("tp")
    other_core = 1 - core
    orders = stage_orders(nbits, groups)

    loads = [
        pltpu.make_async_copy(src, dst, in_sem.at[i])
        for i, (src, dst) in enumerate(
            ((co_hbm, co), (og_hbm, og), (w_hbm, w), (cg_hbm, cg), (cv_hbm, cv))
        )
    ]
    loads[0].start()

    barrier = pltpu.get_barrier_semaphore()

    def greet(i, carry):
        pl.semaphore_signal(
            barrier, inc=1, device_id=(lax.rem(me + i, n), core), device_id_type=MESH
        )
        return carry

    lax.fori_loop(1, n, greet, 0)
    pl.semaphore_signal(barrier, inc=1, device_id=(me, other_core), device_id_type=MESH)

    lane_low = lax.broadcasted_iota(jnp.int32, (1, LANES), 1) < LANES // 2

    gain = gain_ref[...].reshape(1, chan)
    shift = shift_ref[...].reshape(1, chan)
    nt = rows // LANES
    mid = LANES // 2

    def pack(dst):
        for t in range(nt):
            turned = st_a[t * LANES:(t + 1) * LANES, :].T
            dst[0, t:t + 1, :] = turned[:1, :]
            dst[1, t:t + 1, :] = turned[mid:mid + 1, :]

    def unpack(packed, dst):
        for t in range(nt):
            dst[t * LANES:(t + 1) * LANES, :] = jnp.broadcast_to(packed[t:t + 1, :], (LANES, LANES)).T

    def wide(x):
        return jnp.concatenate([x] * cblocks, axis=1)

    loads[0].wait()
    for copy in loads[1:]:
        copy.start()

    def stats(i, carry):
        at = pl.ds(pl.multiple_of(i * 64, 64), 64)
        h = co[at, :].astype(F32)
        mean = jnp.sum(h, axis=1, keepdims=True) / chan
        d = h - mean
        m2 = jnp.sum(d * d, axis=1, keepdims=True)
        st_a[at, :] = jnp.where(lane_low, mean, m2)
        return carry

    repeat(0, rows // 64, stats, 2)
    pack(pk_a)
    pl.semaphore_wait(barrier, n)
    swap_a = pltpu.make_async_remote_copy(
        src_ref=pk_a, dst_ref=pk_b, send_sem=tp_send.at[0], recv_sem=tp_recv.at[0],
        device_id=(me, other_core), device_id_type=MESH,
    )
    swap_a.start()

    loads[1].wait()
    mybits = coordinate_bits(me, nbits)
    sub = LANES // block

    def transpose(c, carry):
        t = og[:, pl.ds(pl.multiple_of(c * LANES, LANES), LANES)].T
        for s in range(sub):
            rbits = coordinate_bits(c * sub + s, nbits)
            piece = t[s * block:(s + 1) * block, :]
            for g in range(groups):
                place = 0
                for k, b in enumerate(orders[g]):
                    place = place + lax.rem(rbits[b] + mybits[b], 2) * (1 << (nbits - 1 - k))
                ogt[g, place] = piece
        return carry

    lax.fori_loop(0, width // LANES, transpose, 0)

    swap_a.wait()
    gap = pk_a[0] - pk_b[0]
    variance = (pk_a[1] + pk_b[1] + gap * gap * (0.5 * chan)) / chan_total
    unpack(0.5 * (pk_a[0] + pk_b[0]), st_b)
    unpack(lax.rsqrt(variance + norm_eps), st_d)

    def norm(i, carry):
        at = pl.ds(pl.multiple_of(i * 32, 32), 32)
        z = (co[at, :].astype(F32) - wide(st_b[at, :])) * wide(st_d[at, :])
        normed[at, :] = z
        x = z * gain + shift
        sig = jax.nn.sigmoid(x)
        active[at, :] = (x * sig).astype(BF16)
        dsilu[at, :] = sig * (1.0 + x * (1.0 - sig))
        return carry

    repeat(0, rows // 32, norm, 2)

    def stage_copy(g, k):
        count = n >> (k + 1)
        off = n - (n >> k)
        return pltpu.make_async_remote_copy(
            src_ref=sendbuf.at[g, pl.ds(off, count)],
            dst_ref=recvbuf.at[g, pl.ds(off, count)],
            send_sem=rs_send.at[g, k],
            recv_sem=rs_recv.at[g, k],
            device_id=(partner_of(me, orders[g][k], nbits), core),
            device_id_type=MESH,
        )

    unit = max(1, n // 4)

    def product(g, start):
        lhs = ogt[g, pl.ds(start, unit)].reshape(unit * block, rows)
        out = jnp.dot(lhs, active[:, g * gcols:(g + 1) * gcols], preferred_element_type=F32)
        return out.reshape(unit, block, gcols)

    for g in range(groups):

        def far(i, carry, g=g):
            sendbuf[g, pl.ds(i * unit, unit)] = product(g, n // 2 + i * unit).astype(BF16)
            return carry

        lax.fori_loop(0, n // 2 // unit, far, 0)
        stage_copy(g, 0).start()
    def stage(k):
        count = n >> (k + 1)
        off = n - (n >> k)
        for g in range(groups):
            stage_copy(g, k).wait_recv()
            if k + 1 < nbits:
                keep = count // 2

                def pass_on(i, carry, g=g):
                    sendbuf[g, off + count + i] = (
                        acc[g, keep + i] + recvbuf[g, off + keep + i].astype(F32)
                    ).astype(BF16)
                    return carry

                lax.fori_loop(0, count - keep, pass_on, 0)
                stage_copy(g, k + 1).start()
            else:
                keep = count

            def take(i, carry, g=g):
                acc[g, i] = acc[g, i] + recvbuf[g, off + i].astype(F32)
                return carry

            lax.fori_loop(0, keep, take, 0)

    loads[2].wait()
    rowacc[...] = jnp.zeros_like(rowacc)

    def act(i, carry):
        at = pl.ds(pl.multiple_of(i * 128, 128), 128)
        scaled[at, :] = jnp.dot(og[at, :], w[...], preferred_element_type=F32)
        return carry

    lax.fori_loop(0, rows // 128, act, 0)

    def grads(i, carry):
        at = pl.ds(pl.multiple_of(i * 32, 32), 32)
        z = normed[at, :]
        ng = scaled[at, :] * dsilu[at, :]
        ngz = ng * z
        rowacc[0] = rowacc[0] + jnp.sum(ngz.reshape(4, 8, chan), axis=0)
        rowacc[1] = rowacc[1] + jnp.sum(ng.reshape(4, 8, chan), axis=0)
        s = ng * gain
        scaled[at, :] = s
        total = jnp.sum(s, axis=1, keepdims=True)
        dot = jnp.sum(s * z, axis=1, keepdims=True)
        st_a[at, :] = jnp.where(lane_low, total, dot)
        return carry

    repeat(0, rows // 32, grads, 2)
    pack(pk_c)
    swap_b = pltpu.make_async_remote_copy(
        src_ref=pk_c, dst_ref=pk_d, send_sem=tp_send.at[1], recv_sem=tp_recv.at[1],
        device_id=(me, other_core), device_id_type=MESH,
    )
    swap_b.start()
    tapacc[...] = jnp.zeros_like(tapacc)
    for c in range(cblocks):
        tapf[c] = taps_ref[:, c * LANES:(c + 1) * LANES].astype(F32)
    flat[...] = jnp.zeros_like(flat)
    for g in range(groups):

        def near(i, carry, g=g):
            acc[g, pl.ds(i * unit, unit)] = product(g, i * unit)
            return carry

        lax.fori_loop(0, n // 2 // unit, near, 0)

    swap_b.wait()
    unpack((pk_c[0] + pk_d[0]) / chan_total, st_a)
    unpack((pk_c[1] + pk_d[1]) / chan_total, st_b)

    def height(i, carry):
        at = pl.ds(pl.multiple_of(i * 32, 32), 32)
        hg = wide(st_d[at, :]) * (
            scaled[at, :] - wide(st_a[at, :]) - normed[at, :] * wide(st_b[at, :])
        )
        for c in range(cblocks):
            hgx[c, at, :] = hg[:, c * LANES:(c + 1) * LANES]
        return carry

    height(0, 0)
    halo_copy = pltpu.make_async_remote_copy(
        src_ref=hgx.at[:, pl.ds(0, halo)],
        dst_ref=hgx.at[:, pl.ds(rows, halo)],
        send_sem=halo_send, recv_sem=halo_recv,
        device_id=(lax.rem(me + n - 1, n), core), device_id_type=MESH,
    )

    @pl.when(me > 0)
    def _():
        halo_copy.start()

    repeat(1, rows // 32, height, 3)

    @pl.when(me == n - 1)
    def _():
        hgx[:, rows:, :] = jnp.zeros((cblocks, halo, LANES), F32)

    loads[3].wait()
    loads[4].wait()
    stage(0)

    @pl.when(me < n - 1)
    def _():
        halo_copy.wait_recv()

    step = 64
    steps = rows // step

    def conv(i, carry):
        c = i // steps
        r = pl.multiple_of(lax.rem(i, steps) * step, step)
        at = pl.ds(r, step)
        cols = pl.ds(pl.multiple_of(c * LANES, LANES), LANES)
        sig = jax.nn.sigmoid(cg[at, cols].astype(F32))
        value = cv[at, cols].astype(F32)
        gated = (value * sig).astype(BF16).astype(F32)
        total = jnp.zeros((step, LANES), F32)
        for j in range(ntaps):
            h = hgx[c, pl.ds(r + reach - j, step), :]
            total = total + tapf[c, pl.ds(j, 1), :] * h
            tapacc[c, j] = tapacc[c, j] + jnp.sum((gated * h).reshape(step // 8, 8, LANES), axis=0)
        gv[at, cols] = (total * sig).astype(BF16)
        gg[at, cols] = (total * value * sig * (1.0 - sig)).astype(BF16)
        return carry

    cut = cblocks * steps * 3 // 4
    lax.fori_loop(0, cut, conv, 0)
    stage(1)
    lax.fori_loop(cut, cblocks * steps, conv, 0)

    for c in range(cblocks):
        rowsum = jnp.sum(tapacc[c], axis=1)
        flat[c * per:c * per + ntaps, :] = rowsum
        for j in range(2):
            flat[c * per + ntaps + j:c * per + ntaps + j + 1, :] = jnp.sum(
                rowacc[j, :, c * LANES:(c + 1) * LANES], axis=0, keepdims=True
            )

    def spread(i):
        peer = lax.rem(me + i, n)
        return pltpu.make_async_remote_copy(
            src_ref=flat.at[pl.ds(pl.multiple_of(peer * chunk, chunk), chunk)],
            dst_ref=parts.at[me],
            send_sem=a_send.at[peer], recv_sem=a_recv.at[me],
            device_id=(peer, core), device_id_type=MESH,
        )

    def collect(i):
        peer = lax.rem(me + i, n)
        return pltpu.make_async_remote_copy(
            src_ref=mine,
            dst_ref=whole.at[pl.ds(pl.multiple_of(me * chunk, chunk), chunk)],
            send_sem=b_send.at[peer], recv_sem=b_recv.at[me],
            device_id=(peer, core), device_id_type=MESH,
        )

    def arrived_part(peer):
        return pltpu.make_async_remote_copy(
            src_ref=flat.at[pl.ds(pl.multiple_of(peer * chunk, chunk), chunk)],
            dst_ref=parts.at[peer],
            send_sem=a_send.at[peer], recv_sem=a_recv.at[peer],
            device_id=(peer, core), device_id_type=MESH,
        )

    def arrived_whole(peer):
        return pltpu.make_async_remote_copy(
            src_ref=mine,
            dst_ref=whole.at[pl.ds(pl.multiple_of(peer * chunk, chunk), chunk)],
            send_sem=b_send.at[peer], recv_sem=b_recv.at[peer],
            device_id=(peer, core), device_id_type=MESH,
        )

    def loop(body):
        def run(i, carry):
            body(i)
            return carry

        lax.fori_loop(1, n, run, 0)

    loop(lambda i: spread(i).start())
    mine[...] = flat[pl.ds(pl.multiple_of(me * chunk, chunk), chunk), :]

    for k in range(2, nbits - 1):
        stage(k)

    def add_part(i):
        peer = lax.rem(me + i, n)
        arrived_part(peer).wait_recv()
        mine[...] = mine[...] + parts[peer]

    loop(add_part)
    loop(lambda i: collect(i).start())
    whole[pl.ds(pl.multiple_of(me * chunk, chunk), chunk), :] = mine[...]

    stage(nbits - 1)
    for g in range(groups):
        proj_out[:, g * gcols:(g + 1) * gcols] = acc[g, 0]
    loop(lambda i: arrived_whole(lax.rem(me + i, n)).wait_recv())
    for c in range(cblocks):
        cols = slice(c * LANES, (c + 1) * LANES)
        taps_out[:, cols] = whole[c * per:c * per + ntaps, :]
        gain_out[cols] = whole[c * per + ntaps, :]
        shift_out[cols] = whole[c * per + ntaps + 1, :]

    loop(lambda i: arrived_part(lax.rem(me + i, n)).wait_send())
    loop(lambda i: arrived_whole(lax.rem(me + i, n)).wait_send())
    for g in range(groups):
        for k in range(nbits):
            stage_copy(g, k).wait_send()

    @pl.when(me > 0)
    def _():
        halo_copy.wait_send()


def place(*refs):
    count = (len(refs) - 1) // 2
    sem = refs[-1]
    copies = [
        pltpu.make_async_copy(src, dst, sem.at[i])
        for i, (src, dst) in enumerate(zip(refs[:count], refs[count:-1]))
    ]
    for copy in copies:
        copy.start()
    for copy in copies:
        copy.wait()


def local(conv_value, conv_gate, conv_out, conv_taps, norm_gain, norm_shift, proj_weight, out_grad):
    rows, chan = conv_value.shape
    ntaps = conv_taps.shape[0]
    width = out_grad.shape[1]
    n = lax.axis_size("sp")
    nbits = n.bit_length() - 1
    assert 1 << nbits == n and lax.axis_size("tp") == 2
    groups = 3
    gcols = chan // groups
    block = width // n
    cblocks = chan // LANES
    halo = 32
    per = -(-(ntaps + 2) // 8) * 8
    chunk = -(-(-(-per * cblocks // n)) // 8) * 8
    dims = (n, nbits, groups, chan * 2)
    hbm = pl.BlockSpec(memory_space=pl.ANY)
    vmem = pl.BlockSpec(memory_space=pltpu.VMEM)
    dma = pltpu.SemaphoreType.DMA
    results = pl.pallas_call(
        functools.partial(kernel, dims),
        out_shape=(
            pltpu.VMEM((rows, chan), BF16),
            pltpu.VMEM((rows, chan), BF16),
            pltpu.VMEM((ntaps, chan), F32),
            pltpu.VMEM((chan,), F32),
            pltpu.VMEM((chan,), F32),
            pltpu.VMEM((block, chan), F32),
        ),
        in_specs=[hbm, hbm, hbm, vmem, vmem, vmem, hbm, hbm],
        out_specs=(vmem,) * 6,
        scratch_shapes=[
            pltpu.VMEM((rows, chan), BF16),
            pltpu.VMEM((rows, chan), BF16),
            pltpu.VMEM((rows, chan), BF16),
            pltpu.VMEM((width, chan), BF16),
            pltpu.VMEM((rows, width), BF16),
            pltpu.VMEM((groups, n, block, rows), BF16),
            pltpu.VMEM((rows, chan), BF16),
            pltpu.VMEM((rows, chan), F32),
            pltpu.VMEM((rows, chan), F32),
            pltpu.VMEM((rows, chan), F32),
            pltpu.VMEM((cblocks, rows + halo, LANES), F32),
            pltpu.VMEM((rows, LANES), F32),
            pltpu.VMEM((rows, LANES), F32),
            pltpu.VMEM((rows, LANES), F32),
            *[pltpu.VMEM((2, rows // LANES, LANES), F32)] * 4,
            pltpu.VMEM((cblocks, ntaps, LANES), F32),
            pltpu.VMEM((groups, n // 2, block, gcols), F32),
            pltpu.VMEM((groups, n, block, gcols), BF16),
            pltpu.VMEM((groups, n, block, gcols), BF16),
            pltpu.VMEM((cblocks, ntaps, 8, LANES), F32),
            pltpu.VMEM((2, 8, chan), F32),
            pltpu.VMEM((n * chunk, LANES), F32),
            pltpu.VMEM((n, chunk, LANES), F32),
            pltpu.VMEM((chunk, LANES), F32),
            pltpu.VMEM((n * chunk, LANES), F32),
            dma((5,)),
            dma((2,)), dma((2,)),
            dma, dma,
            dma((groups, nbits)), dma((groups, nbits)),
            dma((n,)), dma((n,)),
            dma((n,)), dma((n,)),
        ],
        compiler_params=pltpu.CompilerParams(
            collective_id=0, has_side_effects=True, vmem_limit_bytes=60 * 1024 * 1024
        ),
    )(
        conv_value, conv_gate, conv_out, conv_taps, norm_gain, norm_shift, proj_weight, out_grad,
    )
    return pl.pallas_call(
        place,
        out_shape=tuple(jax.ShapeDtypeStruct(x.shape, x.dtype) for x in results),
        in_specs=[vmem] * len(results),
        out_specs=(hbm,) * len(results),
        scratch_shapes=[dma((len(results),))],
    )(*[pltpu.with_memory_space_constraint(x, pltpu.VMEM) for x in results])


def solution(mesh):
    in_specs = (
        P("sp", "tp"),
        P("sp", "tp"),
        P("sp", "tp"),
        P(None, "tp"),
        P("tp"),
        P("tp"),
        P(None, "tp"),
        P("sp", None),
    )
    out_specs = (P("sp", "tp"), P("sp", "tp"), P(None, "tp"), P("tp"), P("tp"), P("sp", "tp"))
    return jax.shard_map(local, mesh=mesh, in_specs=in_specs, out_specs=out_specs, check_vma=False)
```

```python
import functools

import jax
import jax.numpy as jnp
from jax import lax
from jax.experimental import pallas as pl
from jax.experimental.pallas import tpu as pltpu
from jax.sharding import PartitionSpec as P

norm_eps = 1e-05
MESH = pl.DeviceIdType.MESH
F32 = jnp.float32
BF16 = jnp.bfloat16
LANES = 128
HALVES = 4
UNIT = 256
TAP_CUTS = 6
CONV_CUTS = 6
ORDERS = ('ybax', 'xbya', 'byxa', 'xaby', 'xbya', 'xayb', 'yxab', 'ybxa', 'yxba', 'axyb', 'yxab', 'ayxb')
PLAN = [
    ("far", 0), ("send", 0), ("send", 2), ("send", 3), ("far", 1), ("send", 5), ("send", 7), ("far", 2), ("send", 8),
    ("send", 11), ("act", 0), ("act", 1), ("act", 2), ("send", 4), ("send", 6), ("send", 9), ("act", 3), ("grads", 0),
    ("near", 0), ("near", 1), (0, 0), (3, 0), ("near", 2), ("height", 0), ("send", 1), ("send", 10), ("taps", 0),
    ("taps", 1), (5, 0), (7, 0), (11, 0), ("taps", 2), (2, 0), ("taps", 3), ("taps", 4), ("taps", 5), (4, 0), (8, 0),
    (9, 0), ("conv", 0), ("conv", 1), (0, 1), ("edge", 0), (3, 1), (6, 0), ("spread", 0), ("conv", 2), (1, 0), (5, 1),
    ("conv", 3), (8, 1), ("conv", 4), (10, 0), ("conv", 5), (7, 1), (9, 1), (11, 1), ("cedge", 0), (0, 2), (4, 1),
    (6, 1), (2, 1), (3, 2), (5, 2), (10, 1), (9, 2), (7, 2), (4, 2), (11, 2), (3, 3), (1, 1), ("collect", 0), (0, 3),
    (6, 2), (2, 2), (8, 2), (10, 2), (5, 3), (7, 3), (4, 3), (9, 3), (1, 2), (11, 3), (2, 3), (8, 3), (6, 3), (1, 3),
    (10, 3),
]


def repeat(start, stop, body, unroll):
    assert (stop - start) % unroll == 0

    def step(i, carry):
        for u in range(unroll):
            body(start + i * unroll + u, carry)
        return carry

    lax.fori_loop(0, (stop - start) // unroll, step, 0)


def bit(x, b):
    return lax.rem(x // (1 << b), 2)


def split_bits(nbits):
    cuts = [nbits * i // 4 for i in range(5)]
    return [list(range(cuts[i], cuts[i + 1])) for i in range(4)]


def orders_of(nbits, pieces):
    axes = split_bits(nbits)
    names = {"x": axes[0], "y": axes[1], "a": axes[2], "b": axes[3]}
    return [[b for name in ORDERS[p % len(ORDERS)] for b in names[name]] for p in range(pieces)]


def plan_of(nbits, pieces, halves):
    if nbits == 4 and pieces == len(ORDERS):
        return PLAN
    count = pieces // halves
    plan = []
    for g in range(count):
        plan += [("far", g)] + [("send", p) for p in range(g * halves, (g + 1) * halves)]
    plan += [("act", i) for i in range(4)] + [("grads", 0)]
    plan += [("near", g) for g in range(count)] + [("height", 0)]
    plan += [("taps", i) for i in range(TAP_CUTS)] + [("edge", 0), ("spread", 0)]
    for s in range(nbits):
        plan += [(p, s) for p in range(pieces)]
        if s == 0:
            plan += [("conv", i) for i in range(CONV_CUTS)] + [("cedge", 0)]
        if s == nbits - 2:
            plan += [("collect", 0)]
    return plan


def kernel(
    dims,
    cv_hbm, cg_hbm, co_hbm, taps_hbm, gain_hbm, shift_hbm, w_hbm, og_hbm,
    gv, gg, taps_out, gain_out, shift_out, proj_out,
    cv, cg, co, taps_ref, gain_ref, shift_ref, w, og, ogt, active, normed, dsilu, scaled, hgx, halo_out, halo_in,
    st_a, st_b, st_d, pk_a, pk_b, pk_c, pk_d, tapf, acc, sendbuf, recvbuf, tapacc, rowacc, flat, parts, mine, sent, whole,
    in_sem, tp_send, tp_recv, halo_send, halo_recv,
    rs_send, rs_recv, a_send, a_recv, b_send, b_recv, seen,
):
    n, nbits, groups, halves, chan_total = dims
    pieces = groups * halves
    rows, chan = co.shape
    width = og.shape[1]
    block = width // n
    part = block // halves
    gcols = chan // groups
    cblocks = chan // LANES
    gblocks = gcols // LANES
    ntaps = taps_ref.shape[0]
    reach = ntaps - 1
    halo = hgx.shape[1] - rows
    chunk = mine.shape[0]
    per = -(-(ntaps + 2) // 8) * 8
    me = lax.axis_index("sp")
    core = lax.axis_index("tp")
    other_core = 1 - core
    orders = orders_of(nbits, pieces)
    mybits = [bit(me, b) for b in range(nbits)]

    def partner(b):
        return me + (1 << b) * (1 - 2 * mybits[b])

    loads = [
        pltpu.make_async_copy(src, dst, in_sem.at[i])
        for i, (src, dst) in enumerate(
            (
                (co_hbm, co), (og_hbm, og), (w_hbm, w), (cg_hbm, cg), (cv_hbm, cv),
                (gain_hbm, gain_ref), (shift_hbm, shift_ref), (taps_hbm, taps_ref),
            )
        )
    ]
    loads[0].start()
    loads[5].start()
    loads[6].start()
    loads[1].start()

    barrier = pltpu.get_barrier_semaphore()

    def greet(device, c):
        pl.semaphore_signal(barrier, inc=1, device_id=(device, c), device_id_type=MESH)

    greet(me, other_core)
    for b in range(nbits):
        greet(partner(b), core)
    odd = mybits[0]
    beside = me - 1 + 2 * odd
    outside = jnp.where(odd == 1, me == n - 1, me == 0)

    @pl.when(jnp.logical_not(outside))
    def _():
        greet(beside, core)

    lane_low = lax.broadcasted_iota(jnp.int32, (1, LANES), 1) < LANES // 2
    nt = rows // LANES
    mid = LANES // 2

    def pack(dst):
        for t in range(nt):
            turned = st_a[t * LANES:(t + 1) * LANES, :].T
            dst[0, t:t + 1, :] = turned[:1, :]
            dst[1, t:t + 1, :] = turned[mid:mid + 1, :]

    def unpack(packed, dst):
        for t in range(nt):
            dst[t * LANES:(t + 1) * LANES, :] = jnp.broadcast_to(packed[t:t + 1, :], (LANES, LANES)).T

    def wide(x, count):
        return jnp.concatenate([x] * count, axis=1)

    loads[0].wait()
    for copy in loads[2:5] + loads[7:]:
        copy.start()

    def stats(i, carry):
        at = pl.ds(pl.multiple_of(i * 64, 64), 64)
        h = co[at, :].astype(F32)
        mean = jnp.sum(h, axis=1, keepdims=True) / chan
        d = h - mean
        m2 = jnp.sum(d * d, axis=1, keepdims=True)
        st_a[at, :] = jnp.where(lane_low, mean, m2)
        return carry

    repeat(0, rows // 64, stats, 2)
    pack(pk_a)
    pl.semaphore_wait(barrier, jnp.where(outside, nbits + 1, nbits + 2))
    swap_a = pltpu.make_async_remote_copy(
        src_ref=pk_a, dst_ref=pk_b, send_sem=tp_send.at[0], recv_sem=tp_recv.at[0],
        device_id=(me, other_core), device_id_type=MESH,
    )
    swap_a.start()

    def tell(b):
        pl.semaphore_signal(seen.at[b], inc=1, device_id=(partner(b), core), device_id_type=MESH)

    def heard(b):
        pl.semaphore_wait(seen.at[b], 1)
        if b + 2 < nbits:
            tell(b + 1)

    tell(0)
    loads[1].wait()
    sub = LANES // block

    def transpose(c, carry):
        t = og[:, pl.ds(pl.multiple_of(c * LANES, LANES), LANES)].T
        for s in range(sub):
            ogt[c * sub + s] = t[s * block:(s + 1) * block, :]
        return carry

    lax.fori_loop(0, width // LANES, transpose, 0)
    loads[5].wait()
    loads[6].wait()
    gain = gain_ref[...].reshape(1, chan)
    shift = shift_ref[...].reshape(1, chan)
    heard(0)
    swap_a.wait()
    gap = pk_a[0] - pk_b[0]
    variance = (pk_a[1] + pk_b[1] + gap * gap * (0.5 * chan)) / chan_total
    unpack(0.5 * (pk_a[0] + pk_b[0]), st_b)
    unpack(lax.rsqrt(variance + norm_eps), st_d)

    def norm_of(g):
        cols = slice(g * gcols, (g + 1) * gcols)

        def norm(i, carry):
            at = pl.ds(pl.multiple_of(i * 32, 32), 32)
            z = (co[at, cols].astype(F32) - wide(st_b[at, :], gblocks)) * wide(st_d[at, :], gblocks)
            normed[at, cols] = z
            x = z * gain[:, cols] + shift[:, cols]
            sig = jax.nn.sigmoid(x)
            active[at, cols] = (x * sig).astype(BF16)
            dsilu[at, cols] = sig * (1.0 + x * (1.0 - sig))
            return carry

        repeat(0, rows // 32, norm, 4)

    def stage_copy(p, k):
        count = n >> (k + 1)
        off = n - (n >> k)
        return pltpu.make_async_remote_copy(
            src_ref=sendbuf.at[p, pl.ds(off, count)],
            dst_ref=recvbuf.at[p, pl.ds(off, count)],
            send_sem=rs_send.at[p, k],
            recv_sem=rs_recv.at[p, k],
            device_id=(partner(orders[p][k]), core),
            device_id_type=MESH,
        )

    unit = max(1, min(n // 2, UNIT // part))

    def product(p, start):
        g, h = p // halves, p % halves
        found = []
        for i in range(unit):
            place = start + i
            owner = 0
            for k, b in enumerate(orders[p]):
                flip = place >> (nbits - 1 - k) & 1
                owner = owner + (1 - mybits[b] if flip else mybits[b]) * (1 << b)
            found.append(ogt[owner, h * part:(h + 1) * part, :])
        lhs = jnp.concatenate(found, axis=0)
        out = jnp.dot(lhs, active[:, g * gcols:(g + 1) * gcols], preferred_element_type=F32)
        return out.reshape(unit, part, gcols)

    def far(p):
        for i in range(0, n // 2, unit):
            sendbuf[p, i:i + unit] = product(p, n // 2 + i).astype(BF16)

    def near(p):
        for i in range(0, n // 2, unit):
            acc[p, i:i + unit] = product(p, i)

    def arrive(p, k):
        count = n >> (k + 1)
        off = n - (n >> k)
        stage_copy(p, k).wait_recv()
        if k + 1 < nbits:
            keep = count // 2

            def pass_on(i, carry):
                sendbuf[p, off + count + i] = (
                    acc[p, keep + i] + recvbuf[p, off + keep + i].astype(F32)
                ).astype(BF16)
                return carry

            lax.fori_loop(0, count - keep, pass_on, 0)
            stage_copy(p, k + 1).start()

            def take(i, carry):
                acc[p, i] = acc[p, i] + recvbuf[p, off + i].astype(F32)
                return carry

            lax.fori_loop(0, keep, take, 0)
        else:
            g, h = p // halves, p % halves
            proj_out[h * part:(h + 1) * part, g * gcols:(g + 1) * gcols] = (
                acc[p, 0] + recvbuf[p, off].astype(F32)
            )

    def act(i):
        count = rows // 4
        at = slice(i * count, (i + 1) * count)
        scaled[at, :] = jnp.dot(og[at, :], w[...], preferred_element_type=F32)

    def grads(i, carry):
        at = pl.ds(pl.multiple_of(i * 32, 32), 32)
        z = normed[at, :]
        ng = scaled[at, :] * dsilu[at, :]
        ngz = ng * z
        rowacc[0] = rowacc[0] + jnp.sum(ngz.reshape(4, 8, chan), axis=0)
        rowacc[1] = rowacc[1] + jnp.sum(ng.reshape(4, 8, chan), axis=0)
        s = ng * gain
        scaled[at, :] = s
        total = jnp.sum(s, axis=1, keepdims=True)
        dot = jnp.sum(s * z, axis=1, keepdims=True)
        st_a[at, :] = jnp.where(lane_low, total, dot)
        return carry

    def height(i, carry):
        at = pl.ds(pl.multiple_of(i * 32, 32), 32)
        hg = wide(st_d[at, :], cblocks) * (
            scaled[at, :] - wide(st_a[at, :], cblocks) - normed[at, :] * wide(st_b[at, :], cblocks)
        )
        for c in range(cblocks):
            hgx[c, at, :] = hg[:, c * LANES:(c + 1) * LANES]
        return carry

    halo_copy = pltpu.make_async_remote_copy(
        src_ref=halo_out, dst_ref=halo_in,
        send_sem=halo_send, recv_sem=halo_recv,
        device_id=(lax.rem(me + n - 1, n), core), device_id_type=MESH,
    )
    swap_b = pltpu.make_async_remote_copy(
        src_ref=pk_c, dst_ref=pk_d, send_sem=tp_send.at[1], recv_sem=tp_recv.at[1],
        device_id=(me, other_core), device_id_type=MESH,
    )
    step = 64
    steps = rows // step

    def tap_step(c, r):
        at = pl.ds(r, step)
        cols = pl.ds(pl.multiple_of(c * LANES, LANES), LANES)
        sig = jax.nn.sigmoid(cg[at, cols].astype(F32))
        gated = (cv[at, cols].astype(F32) * sig).astype(BF16).astype(F32)
        for j in range(ntaps):
            h = hgx[c, pl.ds(r + reach - j, step), :]
            tapacc[c, j] = tapacc[c, j] + jnp.sum((gated * h).reshape(step // 8, 8, LANES), axis=0)

    def taps_body(i, carry):
        tap_step(i // (steps - 1), pl.multiple_of(lax.rem(i, steps - 1) * step, step))
        return carry

    def taps_edge(c, carry):
        tap_step(c, rows - step)
        rowsum = jnp.sum(tapacc[c], axis=1)
        at = pl.ds(pl.multiple_of(c * per, 8), ntaps)
        flat[at, :] = rowsum
        return carry

    def conv_step(c, r):
        at = pl.ds(r, step)
        cols = pl.ds(pl.multiple_of(c * LANES, LANES), LANES)
        sig = jax.nn.sigmoid(cg[at, cols].astype(F32))
        value = cv[at, cols].astype(F32)
        total = jnp.zeros((step // 8, 8, LANES), F32)
        for j in range(ntaps):
            h = hgx[c, pl.ds(r + reach - j, step), :].reshape(step // 8, 8, LANES)
            total = total + tapf[c, j] * h
        total = total.reshape(step, LANES)
        gv[at, cols] = (total * sig).astype(BF16)
        gg[at, cols] = (total * value * sig * (1.0 - sig)).astype(BF16)

    def conv_body(i, carry):
        conv_step(i // (steps - 1), pl.multiple_of(lax.rem(i, steps - 1) * step, step))
        return carry

    def conv_edge(c, carry):
        conv_step(c, rows - step)
        return carry

    def peer_of(i):
        return lax.rem(me + i, n)

    def rows_of(device):
        return pl.ds(pl.multiple_of(device * chunk, chunk), chunk)

    def spread_copy(peer, slot):
        return pltpu.make_async_remote_copy(
            src_ref=flat.at[rows_of(peer)], dst_ref=parts.at[slot],
            send_sem=a_send.at[peer], recv_sem=a_recv.at[slot],
            device_id=(peer, core), device_id_type=MESH,
        )

    def collect_copy(peer, owner):
        return pltpu.make_async_remote_copy(
            src_ref=sent, dst_ref=whole.at[rows_of(owner)],
            send_sem=b_send.at[peer], recv_sem=b_recv.at[owner],
            device_id=(peer, core), device_id_type=MESH,
        )

    def loop(body):
        def run(i, carry):
            body(peer_of(i))
            return carry

        lax.fori_loop(1, n, run, 0)

    def add_part(peer):
        spread_copy(peer, peer).wait_recv()
        mine[...] = mine[...] + parts[peer]

    taps_total = cblocks * (steps - 1)
    for what, i in plan_of(nbits, pieces, halves):
        if what == "far":
            norm_of(i)
            for p in range(i * halves, (i + 1) * halves):
                far(p)
            if i == 0 and nbits > 2:
                heard(1)
        elif what == "send":
            stage_copy(i, 0).start()
        elif what == "near":
            for p in range(i * halves, (i + 1) * halves):
                near(p)
        elif what == "act":
            if i == 0:
                loads[2].wait()
                rowacc[...] = jnp.zeros_like(rowacc)
            act(i)
        elif what == "grads":
            repeat(0, rows // 32, grads, 2)
            pack(pk_c)
            swap_b.start()
            tapacc[...] = jnp.zeros_like(tapacc)
            loads[7].wait()
            for c in range(cblocks):
                for j in range(ntaps):
                    row = taps_ref[j:j + 1, c * LANES:(c + 1) * LANES].astype(F32)
                    tapf[c, j] = jnp.broadcast_to(row, (8, LANES))
            flat[...] = jnp.zeros_like(flat)
        elif what == "height":
            swap_b.wait()
            unpack((pk_c[0] + pk_d[0]) / chan_total, st_a)
            unpack((pk_c[1] + pk_d[1]) / chan_total, st_b)
            height(0, 0)
            halo_out[...] = hgx[:, :halo, :].astype(BF16)

            @pl.when(me > 0)
            def _():
                halo_copy.start()

            repeat(1, rows // 32, height, 3)
            loads[3].wait()
            loads[4].wait()
        elif what == "taps":
            lax.fori_loop(taps_total * i // TAP_CUTS, taps_total * (i + 1) // TAP_CUTS, taps_body, 0)
        elif what == "edge":
            @pl.when(me < n - 1)
            def _():
                halo_copy.wait_recv()

            hgx[:, rows:, :] = jnp.where(me < n - 1, halo_in[...].astype(F32), 0.0)
            lax.fori_loop(0, cblocks, taps_edge, 0)
            for c in range(cblocks):
                for j in range(2):
                    flat[c * per + ntaps + j:c * per + ntaps + j + 1, :] = jnp.sum(
                        rowacc[j, :, c * LANES:(c + 1) * LANES], axis=0, keepdims=True
                    )
        elif what == "spread":
            for b in range(2, nbits - 1):
                heard(b)
            loop(lambda peer: spread_copy(peer, me).start())
            mine[...] = flat[rows_of(me), :]
        elif what == "collect":
            loop(add_part)
            sent[...] = mine[...].astype(BF16)
            loop(lambda peer: collect_copy(peer, me).start())
            whole[rows_of(me), :] = sent[...]
        elif what == "conv":
            lax.fori_loop(taps_total * i // CONV_CUTS, taps_total * (i + 1) // CONV_CUTS, conv_body, 0)
        elif what == "cedge":
            lax.fori_loop(0, cblocks, conv_edge, 0)
        else:
            arrive(what, i)
    loop(lambda peer: collect_copy(peer, peer).wait_recv())
    for c in range(cblocks):
        cols = slice(c * LANES, (c + 1) * LANES)
        found = whole[c * per:(c + 1) * per, :].astype(F32)
        taps_out[:, cols] = found[:ntaps, :]
        gain_out[cols] = found[ntaps, :]
        shift_out[cols] = found[ntaps + 1, :]

    loop(lambda peer: spread_copy(peer, me).wait_send())
    loop(lambda peer: collect_copy(peer, me).wait_send())
    for p in range(pieces):
        for k in range(nbits):
            stage_copy(p, k).wait_send()

    @pl.when(me > 0)
    def _():
        halo_copy.wait_send()


def place(*refs):
    count = (len(refs) - 1) // 2
    sem = refs[-1]
    copies = [
        pltpu.make_async_copy(src, dst, sem.at[i])
        for i, (src, dst) in enumerate(zip(refs[:count], refs[count:-1]))
    ]
    for copy in copies:
        copy.start()
    for copy in copies:
        copy.wait()


def local(conv_value, conv_gate, conv_out, conv_taps, norm_gain, norm_shift, proj_weight, out_grad):
    rows, chan = conv_value.shape
    ntaps = conv_taps.shape[0]
    width = out_grad.shape[1]
    n = lax.axis_size("sp")
    nbits = n.bit_length() - 1
    assert 1 << nbits == n and lax.axis_size("tp") == 2
    groups = 3
    gcols = chan // groups
    block = width // n
    halves = min(HALVES, block // 8)
    pieces = groups * halves
    part = block // halves
    cblocks = chan // LANES
    halo = 32
    per = -(-(ntaps + 2) // 8) * 8
    chunk = -(-(-(-per * cblocks // n)) // 8) * 8
    dims = (n, nbits, groups, halves, chan * 2)
    hbm = pl.BlockSpec(memory_space=pl.ANY)
    vmem = pl.BlockSpec(memory_space=pltpu.VMEM)
    dma = pltpu.SemaphoreType.DMA
    results = pl.pallas_call(
        functools.partial(kernel, dims),
        out_shape=(
            pltpu.VMEM((rows, chan), BF16),
            pltpu.VMEM((rows, chan), BF16),
            pltpu.VMEM((ntaps, chan), F32),
            pltpu.VMEM((chan,), F32),
            pltpu.VMEM((chan,), F32),
            pltpu.VMEM((block, chan), F32),
        ),
        in_specs=[hbm] * 8,
        out_specs=(vmem,) * 6,
        scratch_shapes=[
            pltpu.VMEM((rows, chan), BF16),
            pltpu.VMEM((rows, chan), BF16),
            pltpu.VMEM((rows, chan), BF16),
            pltpu.VMEM((ntaps, chan), BF16),
            pltpu.VMEM((chan,), F32),
            pltpu.VMEM((chan,), F32),
            pltpu.VMEM((width, chan), BF16),
            pltpu.VMEM((rows, width), BF16),
            pltpu.VMEM((n, block, rows), BF16),
            pltpu.VMEM((rows, chan), BF16),
            pltpu.VMEM((rows, chan), F32),
            pltpu.VMEM((rows, chan), F32),
            pltpu.VMEM((rows, chan), F32),
            pltpu.VMEM((cblocks, rows + halo, LANES), F32),
            pltpu.VMEM((cblocks, halo, LANES), BF16),
            pltpu.VMEM((cblocks, halo, LANES), BF16),
            pltpu.VMEM((rows, LANES), F32),
            pltpu.VMEM((rows, LANES), F32),
            pltpu.VMEM((rows, LANES), F32),
            *[pltpu.VMEM((2, rows // LANES, LANES), F32)] * 4,
            pltpu.VMEM((cblocks, ntaps, 8, LANES), F32),
            pltpu.VMEM((pieces, n // 2, part, gcols), F32),
            pltpu.VMEM((pieces, n, part, gcols), BF16),
            pltpu.VMEM((pieces, n, part, gcols), BF16),
            pltpu.VMEM((cblocks, ntaps, 8, LANES), F32),
            pltpu.VMEM((2, 8, chan), F32),
            pltpu.VMEM((n * chunk, LANES), F32),
            pltpu.VMEM((n, chunk, LANES), F32),
            pltpu.VMEM((chunk, LANES), F32),
            pltpu.VMEM((chunk, LANES), BF16),
            pltpu.VMEM((n * chunk, LANES), BF16),
            dma((8,)),
            dma((2,)), dma((2,)),
            dma, dma,
            dma((pieces, nbits)), dma((pieces, nbits)),
            dma((n,)), dma((n,)),
            dma((n,)), dma((n,)),
            pltpu.SemaphoreType.REGULAR((nbits,)),
        ],
        compiler_params=pltpu.CompilerParams(
            collective_id=0, has_side_effects=True, vmem_limit_bytes=60 * 1024 * 1024
        ),
    )(
        conv_value, conv_gate, conv_out, conv_taps, norm_gain, norm_shift, proj_weight, out_grad,
    )
    return pl.pallas_call(
        place,
        out_shape=tuple(jax.ShapeDtypeStruct(x.shape, x.dtype) for x in results),
        in_specs=[vmem] * len(results),
        out_specs=(hbm,) * len(results),
        scratch_shapes=[dma((len(results),))],
    )(*[pltpu.with_memory_space_constraint(x, pltpu.VMEM) for x in results])


def solution(mesh):
    in_specs = (
        P("sp", "tp"),
        P("sp", "tp"),
        P("sp", "tp"),
        P(None, "tp"),
        P("tp"),
        P("tp"),
        P(None, "tp"),
        P("sp", None),
    )
    out_specs = (P("sp", "tp"), P("sp", "tp"), P(None, "tp"), P("tp"), P("tp"), P("sp", "tp"))
    return jax.shard_map(local, mesh=mesh, in_specs=in_specs, out_specs=out_specs, check_vma=False)
```

```python
import functools

import jax
import jax.numpy as jnp
from jax import lax
from jax.experimental import pallas as pl
from jax.experimental.pallas import tpu as pltpu
from jax.sharding import PartitionSpec as P

norm_eps = 1e-05
MESH = pl.DeviceIdType.MESH
F32 = jnp.float32
BF16 = jnp.bfloat16
LANES = 128
HALVES = 4
UNIT = 256
TAP_CUTS = 6
CONV_CUTS = 6
ORDERS = ('xaby', 'yaxb', 'axby', 'yabx', 'xyab', 'yxab', 'yxab', 'axby', 'yaxb', 'xyab', 'xyab', 'abyx')
PLAN = [
    ("far", 0), ("send", 0), ("send", 1), ("send", 2), ("send", 3), ("far", 1), ("send", 6), ("far", 2), ("send", 10),
    ("send", 11), ("act", 0), ("act", 1), ("act", 2), ("send", 9), ("act", 3), ("grads", 0), ("send", 7), ("send", 8),
    ("near", 0), (0, 0), (1, 0), (2, 0), ("near", 1), ("near", 2), ("height", 0), ("send", 4), ("send", 5),
    ("taps", 0), ("taps", 1), (3, 0), (10, 0), (11, 0), ("taps", 2), ("taps", 3), ("taps", 4), ("taps", 5),
    ("conv", 0), (6, 0), (7, 0), (9, 0), ("conv", 1), (0, 1), (2, 1), ("conv", 2), ("conv", 3), (1, 1), (8, 0),
    ("conv", 4), ("edge", 0), (3, 1), ("spread", 0), ("conv", 5), (4, 0), (5, 0), ("cedge", 0), (11, 1), (6, 1),
    (10, 1), (0, 2), (2, 2), (7, 1), (8, 1), (9, 1), (1, 2), (3, 2), (6, 2), (4, 1), (5, 1), (10, 2), (11, 2), (8, 2),
    (0, 3), (2, 3), ("collect", 0), (3, 3), (9, 2), (7, 2), (1, 3), (11, 3), (4, 2), (6, 3), (5, 2), (7, 3), (10, 3),
    (8, 3), (9, 3), (4, 3), (5, 3),
]


def repeat(start, stop, body, unroll):
    assert (stop - start) % unroll == 0

    def step(i, carry):
        for u in range(unroll):
            body(start + i * unroll + u, carry)
        return carry

    lax.fori_loop(0, (stop - start) // unroll, step, 0)


def bit(x, b):
    return lax.rem(x // (1 << b), 2)


def split_bits(nbits):
    cuts = [nbits * i // 4 for i in range(5)]
    return [list(range(cuts[i], cuts[i + 1])) for i in range(4)]


def orders_of(nbits, pieces):
    axes = split_bits(nbits)
    names = {"x": axes[0], "y": axes[1], "a": axes[2], "b": axes[3]}
    return [[b for name in ORDERS[p % len(ORDERS)] for b in names[name]] for p in range(pieces)]


def plan_of(nbits, pieces, halves):
    if nbits == 4 and pieces == len(ORDERS):
        return PLAN
    count = pieces // halves
    plan = []
    for g in range(count):
        plan += [("far", g)] + [("send", p) for p in range(g * halves, (g + 1) * halves)]
    plan += [("act", i) for i in range(4)] + [("grads", 0)]
    plan += [("near", g) for g in range(count)] + [("height", 0)]
    plan += [("taps", i) for i in range(TAP_CUTS)] + [("edge", 0), ("spread", 0)]
    for s in range(nbits):
        plan += [(p, s) for p in range(pieces)]
        if s == 0:
            plan += [("conv", i) for i in range(CONV_CUTS)] + [("cedge", 0)]
        if s == nbits - 2:
            plan += [("collect", 0)]
    return plan


def kernel(
    dims,
    cv_hbm, cg_hbm, co_hbm, taps_hbm, gain_hbm, shift_hbm, w_hbm, og_hbm,
    gv, gg, taps_out, gain_out, shift_out, proj_out,
    cv, cg, co, taps_ref, gain_ref, shift_ref, w, og, ogt, active, normed, dsilu, scaled, hgx, halo_out, halo_in,
    st_a, st_b, st_d, pk_a, pk_b, pk_c, pk_d, tapf, acc, sendbuf, recvbuf, tapacc, rowacc, flat, narrow, parts, mine, sent, whole,
    in_sem, tp_send, tp_recv, halo_send, halo_recv,
    rs_send, rs_recv, a_send, a_recv, b_send, b_recv, seen,
):
    n, nbits, groups, halves, chan_total = dims
    pieces = groups * halves
    rows, chan = co.shape
    width = og.shape[1]
    block = width // n
    part = block // halves
    gcols = chan // groups
    cblocks = chan // LANES
    gblocks = gcols // LANES
    ntaps = taps_ref.shape[0]
    reach = ntaps - 1
    halo = hgx.shape[1] - rows
    chunk = mine.shape[0]
    per = -(-(ntaps + 2) // 8) * 8
    me = lax.axis_index("sp")
    core = lax.axis_index("tp")
    other_core = 1 - core
    orders = orders_of(nbits, pieces)
    mybits = [bit(me, b) for b in range(nbits)]

    def partner(b):
        return me + (1 << b) * (1 - 2 * mybits[b])

    loads = [
        pltpu.make_async_copy(src, dst, in_sem.at[i])
        for i, (src, dst) in enumerate(
            (
                (co_hbm, co), (og_hbm, og), (w_hbm, w), (cg_hbm, cg), (cv_hbm, cv),
                (gain_hbm, gain_ref), (shift_hbm, shift_ref), (taps_hbm, taps_ref),
            )
        )
    ]
    loads[0].start()
    loads[5].start()
    loads[6].start()
    loads[1].start()

    barrier = pltpu.get_barrier_semaphore()

    def greet(device, c):
        pl.semaphore_signal(barrier, inc=1, device_id=(device, c), device_id_type=MESH)

    greet(me, other_core)
    for b in range(nbits):
        greet(partner(b), core)
    odd = mybits[0]
    beside = me - 1 + 2 * odd
    outside = jnp.where(odd == 1, me == n - 1, me == 0)

    @pl.when(jnp.logical_not(outside))
    def _():
        greet(beside, core)

    lane_low = lax.broadcasted_iota(jnp.int32, (1, LANES), 1) < LANES // 2
    nt = rows // LANES
    mid = LANES // 2

    def pack(dst):
        for t in range(nt):
            turned = st_a[t * LANES:(t + 1) * LANES, :].T
            dst[0, t:t + 1, :] = turned[:1, :]
            dst[1, t:t + 1, :] = turned[mid:mid + 1, :]

    def unpack(packed, dst):
        for t in range(nt):
            dst[t * LANES:(t + 1) * LANES, :] = jnp.broadcast_to(packed[t:t + 1, :], (LANES, LANES)).T

    def wide(x, count):
        return jnp.concatenate([x] * count, axis=1)

    loads[0].wait()
    for copy in loads[2:5] + loads[7:]:
        copy.start()

    def stats(i, carry):
        at = pl.ds(pl.multiple_of(i * 32, 32), 32)
        h = co[at, :].astype(F32)
        mean = jnp.sum(h, axis=1, keepdims=True) / chan
        d = h - mean
        m2 = jnp.sum(d * d, axis=1, keepdims=True)
        st_a[at, :] = jnp.where(lane_low, mean, m2)
        return carry

    repeat(0, rows // 32, stats, 8)
    pack(pk_a)
    pl.semaphore_wait(barrier, jnp.where(outside, nbits + 1, nbits + 2))
    swap_a = pltpu.make_async_remote_copy(
        src_ref=pk_a, dst_ref=pk_b, send_sem=tp_send.at[0], recv_sem=tp_recv.at[0],
        device_id=(me, other_core), device_id_type=MESH,
    )
    swap_a.start()

    def tell(b):
        pl.semaphore_signal(seen.at[b], inc=1, device_id=(partner(b), core), device_id_type=MESH)

    def heard(b):
        pl.semaphore_wait(seen.at[b], 1)
        if b + 2 < nbits:
            tell(b + 1)

    tell(0)
    loads[1].wait()
    sub = LANES // block

    def transpose(c, carry):
        t = og[:, pl.ds(pl.multiple_of(c * LANES, LANES), LANES)].T
        for s in range(sub):
            ogt[c * sub + s] = t[s * block:(s + 1) * block, :]
        return carry

    lax.fori_loop(0, width // LANES, transpose, 0)
    loads[5].wait()
    loads[6].wait()
    gain = gain_ref[...].reshape(1, chan)
    shift = shift_ref[...].reshape(1, chan)
    heard(0)
    swap_a.wait()
    gap = pk_a[0] - pk_b[0]
    variance = (pk_a[1] + pk_b[1] + gap * gap * (0.5 * chan)) / chan_total
    unpack(0.5 * (pk_a[0] + pk_b[0]), st_b)
    unpack(lax.rsqrt(variance + norm_eps), st_d)

    def norm_of(g):
        cols = slice(g * gcols, (g + 1) * gcols)

        def norm(i, carry):
            at = pl.ds(pl.multiple_of(i * 32, 32), 32)
            z = (co[at, cols].astype(F32) - wide(st_b[at, :], gblocks)) * wide(st_d[at, :], gblocks)
            normed[at, cols] = z
            x = z * gain[:, cols] + shift[:, cols]
            sig = jax.nn.sigmoid(x)
            active[at, cols] = (x * sig).astype(BF16)
            dsilu[at, cols] = sig * (1.0 + x * (1.0 - sig))
            return carry

        repeat(0, rows // 32, norm, 4)

    def stage_copy(p, k):
        count = n >> (k + 1)
        off = n - (n >> k)
        return pltpu.make_async_remote_copy(
            src_ref=sendbuf.at[p, pl.ds(off, count)],
            dst_ref=recvbuf.at[p, pl.ds(off, count)],
            send_sem=rs_send,
            recv_sem=rs_recv.at[p, k],
            device_id=(partner(orders[p][k]), core),
            device_id_type=MESH,
        )

    unit = max(1, min(n // 2, UNIT // part))

    def product(p, start):
        g, h = p // halves, p % halves
        found = []
        for i in range(unit):
            place = start + i
            owner = 0
            for k, b in enumerate(orders[p]):
                flip = place >> (nbits - 1 - k) & 1
                owner = owner + (1 - mybits[b] if flip else mybits[b]) * (1 << b)
            found.append(ogt[owner, h * part:(h + 1) * part, :])
        lhs = jnp.concatenate(found, axis=0)
        out = jnp.dot(lhs, active[:, g * gcols:(g + 1) * gcols], preferred_element_type=F32)
        return out.reshape(unit, part, gcols)

    def far(p):
        for i in range(0, n // 2, unit):
            sendbuf[p, i:i + unit] = product(p, n // 2 + i).astype(BF16)

    def near(p):
        for i in range(0, n // 2, unit):
            acc[p, i:i + unit] = product(p, i)

    def arrive(p, k):
        count = n >> (k + 1)
        off = n - (n >> k)
        stage_copy(p, k).wait_recv()
        if k + 1 < nbits:
            keep = count // 2

            def pass_on(i, carry):
                sendbuf[p, off + count + i] = (
                    acc[p, keep + i] + recvbuf[p, off + keep + i].astype(F32)
                ).astype(BF16)
                return carry

            lax.fori_loop(0, count - keep, pass_on, 0)
            stage_copy(p, k + 1).start()

            def take(i, carry):
                acc[p, i] = acc[p, i] + recvbuf[p, off + i].astype(F32)
                return carry

            lax.fori_loop(0, keep, take, 0)
        else:
            g, h = p // halves, p % halves
            proj_out[h * part:(h + 1) * part, g * gcols:(g + 1) * gcols] = (
                acc[p, 0] + recvbuf[p, off].astype(F32)
            )

    def act(i):
        count = rows // 4
        at = slice(i * count, (i + 1) * count)
        scaled[at, :] = jnp.dot(og[at, :], w[...], preferred_element_type=F32)

    def grads(i, carry):
        at = pl.ds(pl.multiple_of(i * 32, 32), 32)
        z = normed[at, :]
        ng = scaled[at, :] * dsilu[at, :]
        ngz = ng * z
        rowacc[0] = rowacc[0] + jnp.sum(ngz.reshape(4, 8, chan), axis=0)
        rowacc[1] = rowacc[1] + jnp.sum(ng.reshape(4, 8, chan), axis=0)
        s = ng * gain
        scaled[at, :] = s
        total = jnp.sum(s, axis=1, keepdims=True)
        dot = jnp.sum(s * z, axis=1, keepdims=True)
        st_a[at, :] = jnp.where(lane_low, total, dot)
        return carry

    def height(i, carry):
        at = pl.ds(pl.multiple_of(i * 32, 32), 32)
        hg = wide(st_d[at, :], cblocks) * (
            scaled[at, :] - wide(st_a[at, :], cblocks) - normed[at, :] * wide(st_b[at, :], cblocks)
        )
        for c in range(cblocks):
            hgx[c, at, :] = hg[:, c * LANES:(c + 1) * LANES]
        return carry

    halo_copy = pltpu.make_async_remote_copy(
        src_ref=halo_out, dst_ref=halo_in,
        send_sem=halo_send, recv_sem=halo_recv,
        device_id=(lax.rem(me + n - 1, n), core), device_id_type=MESH,
    )
    swap_b = pltpu.make_async_remote_copy(
        src_ref=pk_c, dst_ref=pk_d, send_sem=tp_send.at[1], recv_sem=tp_recv.at[1],
        device_id=(me, other_core), device_id_type=MESH,
    )
    step = 64
    steps = rows // step

    def tap_step(c, r):
        at = pl.ds(r, step)
        cols = pl.ds(pl.multiple_of(c * LANES, LANES), LANES)
        sig = jax.nn.sigmoid(cg[at, cols].astype(F32))
        gated = (cv[at, cols].astype(F32) * sig).astype(BF16).astype(F32)
        for j in range(ntaps):
            h = hgx[c, pl.ds(r + reach - j, step), :]
            tapacc[c, j] = tapacc[c, j] + jnp.sum((gated * h).reshape(step // 8, 8, LANES), axis=0)

    def taps_body(i, carry):
        tap_step(i // (steps - 1), pl.multiple_of(lax.rem(i, steps - 1) * step, step))
        return carry

    def taps_edge(c, carry):
        tap_step(c, rows - step)
        rowsum = jnp.sum(tapacc[c], axis=1)
        at = pl.ds(pl.multiple_of(c * per, 8), ntaps)
        flat[at, :] = rowsum
        return carry

    def conv_step(c, r):
        at = pl.ds(r, step)
        cols = pl.ds(pl.multiple_of(c * LANES, LANES), LANES)
        sig = jax.nn.sigmoid(cg[at, cols].astype(F32))
        value = cv[at, cols].astype(F32)
        total = jnp.zeros((step // 8, 8, LANES), F32)
        for j in range(ntaps):
            h = hgx[c, pl.ds(r + reach - j, step), :].reshape(step // 8, 8, LANES)
            total = total + tapf[c, j] * h
        total = total.reshape(step, LANES)
        gv[at, cols] = (total * sig).astype(BF16)
        gg[at, cols] = (total * value * sig * (1.0 - sig)).astype(BF16)

    def conv_body(i, carry):
        conv_step(i // (steps - 1), pl.multiple_of(lax.rem(i, steps - 1) * step, step))
        return carry

    def conv_edge(c, carry):
        conv_step(c, rows - step)
        return carry

    def peer_of(i):
        return lax.rem(me + i, n)

    def rows_of(device):
        return pl.ds(pl.multiple_of(device * chunk, chunk), chunk)

    def spread_copy(peer, slot):
        return pltpu.make_async_remote_copy(
            src_ref=narrow.at[rows_of(peer)], dst_ref=parts.at[slot],
            send_sem=a_send, recv_sem=a_recv,
            device_id=(peer, core), device_id_type=MESH,
        )

    def collect_copy(peer, owner):
        return pltpu.make_async_remote_copy(
            src_ref=sent, dst_ref=whole.at[rows_of(owner)],
            send_sem=b_send, recv_sem=b_recv,
            device_id=(peer, core), device_id_type=MESH,
        )

    def loop(body):
        def run(i, carry):
            body(peer_of(i))
            return carry

        lax.fori_loop(1, n, run, 0)

    def add_part(peer):
        mine[...] = mine[...] + parts[peer].astype(F32)

    def all_of(buffer, send_sem, recv_sem):
        return pltpu.make_async_remote_copy(
            src_ref=buffer, dst_ref=buffer, send_sem=send_sem, recv_sem=recv_sem,
            device_id=(me, other_core), device_id_type=MESH,
        )

    all_parts = all_of(parts.at[pl.ds(0, n - 1)], a_send, a_recv)
    all_whole = all_of(whole.at[pl.ds(0, (n - 1) * chunk)], b_send, b_recv)
    all_pieces = all_of(sendbuf.at[:, pl.ds(0, n - 1)], rs_send, rs_recv.at[0, 0])

    taps_total = cblocks * (steps - 1)
    for what, i in plan_of(nbits, pieces, halves):
        if what == "far":
            norm_of(i)
            for p in range(i * halves, (i + 1) * halves):
                far(p)
            if i == 0 and nbits > 2:
                heard(1)
        elif what == "send":
            stage_copy(i, 0).start()
        elif what == "near":
            for p in range(i * halves, (i + 1) * halves):
                near(p)
        elif what == "act":
            if i == 0:
                loads[2].wait()
                rowacc[...] = jnp.zeros_like(rowacc)
            act(i)
        elif what == "grads":
            repeat(0, rows // 32, grads, 2)
            pack(pk_c)
            swap_b.start()
            tapacc[...] = jnp.zeros_like(tapacc)
            loads[7].wait()
            for c in range(cblocks):
                for j in range(ntaps):
                    row = taps_ref[j:j + 1, c * LANES:(c + 1) * LANES].astype(F32)
                    tapf[c, j] = jnp.broadcast_to(row, (8, LANES))
            flat[...] = jnp.zeros_like(flat)
        elif what == "height":
            swap_b.wait()
            unpack((pk_c[0] + pk_d[0]) / chan_total, st_a)
            unpack((pk_c[1] + pk_d[1]) / chan_total, st_b)
            height(0, 0)
            halo_out[...] = hgx[:, :halo, :].astype(BF16)

            @pl.when(me > 0)
            def _():
                halo_copy.start()

            repeat(1, rows // 32, height, 3)
            loads[3].wait()
            loads[4].wait()
        elif what == "taps":
            lax.fori_loop(taps_total * i // TAP_CUTS, taps_total * (i + 1) // TAP_CUTS, taps_body, 0, unroll=7)
        elif what == "edge":
            @pl.when(me < n - 1)
            def _():
                halo_copy.wait_recv()

            hgx[:, rows:, :] = jnp.where(me < n - 1, halo_in[...].astype(F32), 0.0)
            lax.fori_loop(0, cblocks, taps_edge, 0, unroll=3)
            for c in range(cblocks):
                for j in range(2):
                    flat[c * per + ntaps + j:c * per + ntaps + j + 1, :] = jnp.sum(
                        rowacc[j, :, c * LANES:(c + 1) * LANES], axis=0, keepdims=True
                    )
        elif what == "spread":
            for b in range(2, nbits - 1):
                heard(b)
            narrow[...] = flat[...].astype(BF16)
            loop(lambda peer: spread_copy(peer, me).start())
            mine[...] = flat[rows_of(me), :]
        elif what == "collect":
            all_parts.wait_recv()
            loop(add_part)
            sent[...] = mine[...].astype(BF16)
            loop(lambda peer: collect_copy(peer, me).start())
            whole[rows_of(me), :] = sent[...]
        elif what == "conv":
            lax.fori_loop(taps_total * i // CONV_CUTS, taps_total * (i + 1) // CONV_CUTS, conv_body, 0, unroll=7)
        elif what == "cedge":
            lax.fori_loop(0, cblocks, conv_edge, 0, unroll=3)
        else:
            arrive(what, i)
    all_whole.wait_recv()
    for c in range(cblocks):
        cols = slice(c * LANES, (c + 1) * LANES)
        found = whole[c * per:(c + 1) * per, :].astype(F32)
        taps_out[:, cols] = found[:ntaps, :]
        gain_out[cols] = found[ntaps, :]
        shift_out[cols] = found[ntaps + 1, :]

    all_parts.wait_send()
    all_whole.wait_send()
    all_pieces.wait_send()

    @pl.when(me > 0)
    def _():
        halo_copy.wait_send()


def place(*refs):
    count = (len(refs) - 1) // 2
    sem = refs[-1]
    copies = [
        pltpu.make_async_copy(src, dst, sem.at[i])
        for i, (src, dst) in enumerate(zip(refs[:count], refs[count:-1]))
    ]
    for copy in copies:
        copy.start()
    for copy in copies:
        copy.wait()


def local(conv_value, conv_gate, conv_out, conv_taps, norm_gain, norm_shift, proj_weight, out_grad):
    rows, chan = conv_value.shape
    ntaps = conv_taps.shape[0]
    width = out_grad.shape[1]
    n = lax.axis_size("sp")
    nbits = n.bit_length() - 1
    assert 1 << nbits == n and lax.axis_size("tp") == 2
    groups = 3
    gcols = chan // groups
    block = width // n
    halves = min(HALVES, block // 8)
    pieces = groups * halves
    part = block // halves
    cblocks = chan // LANES
    halo = 32
    per = -(-(ntaps + 2) // 8) * 8
    chunk = -(-(-(-per * cblocks // n)) // 16) * 16
    dims = (n, nbits, groups, halves, chan * 2)
    hbm = pl.BlockSpec(memory_space=pl.ANY)
    vmem = pl.BlockSpec(memory_space=pltpu.VMEM)
    dma = pltpu.SemaphoreType.DMA
    results = pl.pallas_call(
        functools.partial(kernel, dims),
        out_shape=(
            pltpu.VMEM((rows, chan), BF16),
            pltpu.VMEM((rows, chan), BF16),
            pltpu.VMEM((ntaps, chan), F32),
            pltpu.VMEM((chan,), F32),
            pltpu.VMEM((chan,), F32),
            pltpu.VMEM((block, chan), F32),
        ),
        in_specs=[hbm] * 8,
        out_specs=(vmem,) * 6,
        scratch_shapes=[
            pltpu.VMEM((rows, chan), BF16),
            pltpu.VMEM((rows, chan), BF16),
            pltpu.VMEM((rows, chan), BF16),
            pltpu.VMEM((ntaps, chan), BF16),
            pltpu.VMEM((chan,), F32),
            pltpu.VMEM((chan,), F32),
            pltpu.VMEM((width, chan), BF16),
            pltpu.VMEM((rows, width), BF16),
            pltpu.VMEM((n, block, rows), BF16),
            pltpu.VMEM((rows, chan), BF16),
            pltpu.VMEM((rows, chan), F32),
            pltpu.VMEM((rows, chan), F32),
            pltpu.VMEM((rows, chan), F32),
            pltpu.VMEM((cblocks, rows + halo, LANES), F32),
            pltpu.VMEM((cblocks, halo, LANES), BF16),
            pltpu.VMEM((cblocks, halo, LANES), BF16),
            pltpu.VMEM((rows, LANES), F32),
            pltpu.VMEM((rows, LANES), F32),
            pltpu.VMEM((rows, LANES), F32),
            *[pltpu.VMEM((2, rows // LANES, LANES), F32)] * 4,
            pltpu.VMEM((cblocks, ntaps, 8, LANES), F32),
            pltpu.VMEM((pieces, n // 2, part, gcols), F32),
            pltpu.VMEM((pieces, n, part, gcols), BF16),
            pltpu.VMEM((pieces, n, part, gcols), BF16),
            pltpu.VMEM((cblocks, ntaps, 8, LANES), F32),
            pltpu.VMEM((2, 8, chan), F32),
            pltpu.VMEM((n * chunk, LANES), F32),
            pltpu.VMEM((n * chunk, LANES), BF16),
            pltpu.VMEM((n, chunk, LANES), BF16),
            pltpu.VMEM((chunk, LANES), F32),
            pltpu.VMEM((chunk, LANES), BF16),
            pltpu.VMEM((n * chunk, LANES), BF16),
            dma((8,)),
            dma((2,)), dma((2,)),
            dma, dma,
            dma, dma((pieces, nbits)),
            dma, dma,
            dma, dma,
            pltpu.SemaphoreType.REGULAR((nbits,)),
        ],
        compiler_params=pltpu.CompilerParams(
            collective_id=0, has_side_effects=True, vmem_limit_bytes=60 * 1024 * 1024
        ),
    )(
        conv_value, conv_gate, conv_out, conv_taps, norm_gain, norm_shift, proj_weight, out_grad,
    )
    return pl.pallas_call(
        place,
        out_shape=tuple(jax.ShapeDtypeStruct(x.shape, x.dtype) for x in results),
        in_specs=[vmem] * len(results),
        out_specs=(hbm,) * len(results),
        scratch_shapes=[dma((len(results),))],
    )(*[pltpu.with_memory_space_constraint(x, pltpu.VMEM) for x in results])


def solution(mesh):
    in_specs = (
        P("sp", "tp"),
        P("sp", "tp"),
        P("sp", "tp"),
        P(None, "tp"),
        P("tp"),
        P("tp"),
        P(None, "tp"),
        P("sp", None),
    )
    out_specs = (P("sp", "tp"), P("sp", "tp"), P(None, "tp"), P("tp"), P("tp"), P("sp", "tp"))
    return jax.shard_map(local, mesh=mesh, in_specs=in_specs, out_specs=out_specs, check_vma=False)
```

```python
import functools

import jax
import jax.numpy as jnp
from jax import lax
from jax.experimental import pallas as pl
from jax.experimental.pallas import tpu as pltpu
from jax.sharding import PartitionSpec as P

norm_eps = 1e-05
MESH = pl.DeviceIdType.MESH
F32 = jnp.float32
BF16 = jnp.bfloat16
LANES = 128
HALVES = 4
UNIT = 256
TAP_CUTS = 6
CONV_CUTS = 6
ORDERS = ('byxa', 'yaxb', 'abyx', 'yxba', 'yxab', 'xyba', 'xbya', 'yabx', 'axyb', 'xayb', 'xayb', 'ybxa')
PLAN = [
    ("far", 0), ("send", 0), ("send", 1), ("send", 2), ("far", 1), ("send", 7), ("send", 6), ("far", 2), ("send", 8),
    ("act", 0), ("send", 5), ("act", 1), ("act", 2), ("send", 10), ("act", 3), ("send", 11), ("grads", 0),
    ("near", 2), ("near", 0), ("near", 1), (1, 0), ("height", 0), (6, 0), ("taps", 0), ("conv", 0), ("send", 9),
    ("taps", 1), ("send", 3), ("taps", 2), ("conv", 1), ("taps", 3), ("send", 4), (0, 0), (2, 0), (7, 0), ("taps", 4),
    (8, 0), ("taps", 5), (11, 0), (10, 0), ("conv", 2), (5, 0), (1, 1), ("conv", 3), ("edge", 0), (3, 0),
    ("spread", 0), (6, 1), (4, 0), (9, 0), (7, 1), (8, 1), (2, 1), ("conv", 4), ("conv", 5), (0, 1), (3, 1),
    ("cedge", 0), (11, 1), (10, 1), (1, 2), (5, 1), (6, 2), (4, 1), (0, 2), (8, 2), (2, 2), ("collect", 0), (7, 2),
    (9, 1), (10, 2), (11, 2), (6, 3), (3, 2), (9, 2), (2, 3), (4, 2), (5, 2), (8, 3), (1, 3), (0, 3), (3, 3), (10, 3),
    (11, 3), (7, 3), (9, 3), (5, 3), (4, 3),
]


def repeat(start, stop, body, unroll):
    assert (stop - start) % unroll == 0

    def step(i, carry):
        for u in range(unroll):
            body(start + i * unroll + u, carry)
        return carry

    lax.fori_loop(0, (stop - start) // unroll, step, 0)


def bit(x, b):
    return lax.rem(x // (1 << b), 2)


def split_bits(nbits):
    cuts = [nbits * i // 4 for i in range(5)]
    return [list(range(cuts[i], cuts[i + 1])) for i in range(4)]


def orders_of(nbits, pieces):
    axes = split_bits(nbits)
    names = {"x": axes[0], "y": axes[1], "a": axes[2], "b": axes[3]}
    return [[b for name in ORDERS[p % len(ORDERS)] for b in names[name]] for p in range(pieces)]


def plan_of(nbits, pieces, halves):
    if nbits == 4 and pieces == len(ORDERS):
        return PLAN
    count = pieces // halves
    plan = []
    for g in range(count):
        plan += [("far", g)] + [("send", p) for p in range(g * halves, (g + 1) * halves)]
    plan += [("act", i) for i in range(4)] + [("grads", 0)]
    plan += [("near", g) for g in range(count)] + [("height", 0)]
    plan += [("taps", i) for i in range(TAP_CUTS)] + [("edge", 0), ("spread", 0)]
    for s in range(nbits):
        plan += [(p, s) for p in range(pieces)]
        if s == 0:
            plan += [("conv", i) for i in range(CONV_CUTS)] + [("cedge", 0)]
        if s == nbits - 2:
            plan += [("collect", 0)]
    return plan


def kernel(
    dims,
    cv_hbm, cg_hbm, co_hbm, taps_hbm, gain_hbm, shift_hbm, w_hbm, og_hbm,
    gv, gg, taps_out, gain_out, shift_out, proj_out,
    cv, cg, co, taps_ref, gain_ref, shift_ref, w, og, ogt, active, normed, dsilu, scaled, hgx, halo_out, halo_in,
    st_a, st_b, st_d, pk_a, pk_b, pk_c, pk_d, tapf, acc, sendbuf, recvbuf, tapacc, rowacc, flat, narrow, parts, mine, sent, whole,
    in_sem, tp_send, tp_recv, halo_send, halo_recv,
    rs_send, rs_recv, a_send, a_recv, b_send, b_recv, seen,
):
    n, nbits, groups, halves, chan_total = dims
    pieces = groups * halves
    rows, chan = co.shape
    width = og.shape[1]
    block = width // n
    part = block // halves
    gcols = chan // groups
    cblocks = chan // LANES
    gblocks = gcols // LANES
    ntaps = taps_ref.shape[0]
    reach = ntaps - 1
    halo = hgx.shape[1] - rows
    chunk = mine.shape[0]
    per = -(-(ntaps + 2) // 8) * 8
    me = lax.axis_index("sp")
    core = lax.axis_index("tp")
    other_core = 1 - core
    orders = orders_of(nbits, pieces)
    mybits = [bit(me, b) for b in range(nbits)]

    def partner(b):
        return me + (1 << b) * (1 - 2 * mybits[b])

    loads = [
        pltpu.make_async_copy(src, dst, in_sem.at[i])
        for i, (src, dst) in enumerate(
            (
                (co_hbm, co), (og_hbm, og), (w_hbm, w), (cg_hbm, cg), (cv_hbm, cv),
                (gain_hbm, gain_ref), (shift_hbm, shift_ref), (taps_hbm, taps_ref),
            )
        )
    ]
    loads[0].start()
    loads[5].start()
    loads[6].start()
    loads[1].start()

    barrier = pltpu.get_barrier_semaphore()

    def greet(device, c):
        pl.semaphore_signal(barrier, inc=1, device_id=(device, c), device_id_type=MESH)

    greet(me, other_core)
    for b in range(nbits):
        greet(partner(b), core)
    odd = mybits[0]
    beside = me - 1 + 2 * odd
    outside = jnp.where(odd == 1, me == n - 1, me == 0)

    @pl.when(jnp.logical_not(outside))
    def _():
        greet(beside, core)

    lane_low = lax.broadcasted_iota(jnp.int32, (1, LANES), 1) < LANES // 2
    nt = rows // LANES
    mid = LANES // 2

    def pack(dst):
        for t in range(nt):
            turned = st_a[t * LANES:(t + 1) * LANES, :].T
            dst[0, t:t + 1, :] = turned[:1, :]
            dst[1, t:t + 1, :] = turned[mid:mid + 1, :]

    def unpack(packed, dst):
        for t in range(nt):
            dst[t * LANES:(t + 1) * LANES, :] = jnp.broadcast_to(packed[t:t + 1, :], (LANES, LANES)).T

    def wide(x, count):
        return jnp.concatenate([x] * count, axis=1)

    loads[0].wait()
    for copy in loads[2:5] + loads[7:]:
        copy.start()

    def stats(i, carry):
        at = pl.ds(pl.multiple_of(i * 32, 32), 32)
        h = co[at, :].astype(F32)
        mean = jnp.sum(h, axis=1, keepdims=True) / chan
        d = h - mean
        m2 = jnp.sum(d * d, axis=1, keepdims=True)
        st_a[at, :] = jnp.where(lane_low, mean, m2)
        return carry

    repeat(0, rows // 32, stats, 8)
    pack(pk_a)
    pl.semaphore_wait(barrier, jnp.where(outside, nbits + 1, nbits + 2))
    swap_a = pltpu.make_async_remote_copy(
        src_ref=pk_a, dst_ref=pk_b, send_sem=tp_send.at[0], recv_sem=tp_recv.at[0],
        device_id=(me, other_core), device_id_type=MESH,
    )
    swap_a.start()

    def tell(b):
        pl.semaphore_signal(seen.at[b], inc=1, device_id=(partner(b), core), device_id_type=MESH)

    def heard(b):
        pl.semaphore_wait(seen.at[b], 1)
        if b + 2 < nbits:
            tell(b + 1)

    tell(0)
    loads[1].wait()
    sub = LANES // block

    def transpose(c, carry):
        t = og[:, pl.ds(pl.multiple_of(c * LANES, LANES), LANES)].T
        for s in range(sub):
            ogt[c * sub + s] = t[s * block:(s + 1) * block, :]
        return carry

    lax.fori_loop(0, width // LANES, transpose, 0, unroll=4)
    loads[5].wait()
    loads[6].wait()
    gain = gain_ref[...].reshape(1, chan)
    shift = shift_ref[...].reshape(1, chan)
    swap_a.wait()
    gap = pk_a[0] - pk_b[0]
    variance = (pk_a[1] + pk_b[1] + gap * gap * (0.5 * chan)) / chan_total
    unpack(0.5 * (pk_a[0] + pk_b[0]), st_b)
    unpack(lax.rsqrt(variance + norm_eps), st_d)

    def norm_of(g):
        cols = slice(g * gcols, (g + 1) * gcols)

        def norm(i, carry):
            at = pl.ds(pl.multiple_of(i * 32, 32), 32)
            z = (co[at, cols].astype(F32) - wide(st_b[at, :], gblocks)) * wide(st_d[at, :], gblocks)
            normed[at, cols] = z
            x = z * gain[:, cols] + shift[:, cols]
            sig = jax.nn.sigmoid(x)
            active[at, cols] = (x * sig).astype(BF16)
            dsilu[at, cols] = sig * (1.0 + x * (1.0 - sig))
            return carry

        repeat(0, rows // 32, norm, 4)

    def stage_copy(p, k):
        count = n >> (k + 1)
        off = n - (n >> k)
        return pltpu.make_async_remote_copy(
            src_ref=sendbuf.at[p, pl.ds(off, count)],
            dst_ref=recvbuf.at[p, pl.ds(off, count)],
            send_sem=rs_send,
            recv_sem=rs_recv.at[p, k],
            device_id=(partner(orders[p][k]), core),
            device_id_type=MESH,
        )

    unit = max(1, min(n // 2, UNIT // part))

    def product(p, start):
        g, h = p // halves, p % halves
        found = []
        for i in range(unit):
            place = start + i
            owner = 0
            for k, b in enumerate(orders[p]):
                flip = place >> (nbits - 1 - k) & 1
                owner = owner + (1 - mybits[b] if flip else mybits[b]) * (1 << b)
            found.append(ogt[owner, h * part:(h + 1) * part, :])
        lhs = jnp.concatenate(found, axis=0)
        out = jnp.dot(lhs, active[:, g * gcols:(g + 1) * gcols], preferred_element_type=F32)
        return out.reshape(unit, part, gcols)

    def far(p):
        for i in range(0, n // 2, unit):
            sendbuf[p, i:i + unit] = product(p, n // 2 + i).astype(BF16)

    def near(p):
        for i in range(0, n // 2, unit):
            acc[p, i:i + unit] = product(p, i)

    def arrive(p, k):
        count = n >> (k + 1)
        off = n - (n >> k)
        stage_copy(p, k).wait_recv()
        if k + 1 < nbits:
            keep = count // 2

            def pass_on(i, carry):
                sendbuf[p, off + count + i] = (
                    acc[p, keep + i] + recvbuf[p, off + keep + i].astype(F32)
                ).astype(BF16)
                return carry

            lax.fori_loop(0, count - keep, pass_on, 0)
            stage_copy(p, k + 1).start()

            def take(i, carry):
                acc[p, i] = acc[p, i] + recvbuf[p, off + i].astype(F32)
                return carry

            lax.fori_loop(0, keep, take, 0)
        else:
            g, h = p // halves, p % halves
            proj_out[h * part:(h + 1) * part, g * gcols:(g + 1) * gcols] = (
                acc[p, 0] + recvbuf[p, off].astype(F32)
            )

    def act(i):
        count = rows // 4
        at = slice(i * count, (i + 1) * count)
        scaled[at, :] = jnp.dot(og[at, :], w[...], preferred_element_type=F32)

    def grads(i, carry):
        at = pl.ds(pl.multiple_of(i * 32, 32), 32)
        z = normed[at, :]
        ng = scaled[at, :] * dsilu[at, :]
        ngz = ng * z
        rowacc[0] = rowacc[0] + jnp.sum(ngz.reshape(4, 8, chan), axis=0)
        rowacc[1] = rowacc[1] + jnp.sum(ng.reshape(4, 8, chan), axis=0)
        s = ng * gain
        scaled[at, :] = s
        total = jnp.sum(s, axis=1, keepdims=True)
        dot = jnp.sum(s * z, axis=1, keepdims=True)
        st_a[at, :] = jnp.where(lane_low, total, dot)
        return carry

    def height(i, carry):
        at = pl.ds(pl.multiple_of(i * 32, 32), 32)
        hg = wide(st_d[at, :], cblocks) * (
            scaled[at, :] - wide(st_a[at, :], cblocks) - normed[at, :] * wide(st_b[at, :], cblocks)
        )
        for c in range(cblocks):
            hgx[c, at, :] = hg[:, c * LANES:(c + 1) * LANES]
        return carry

    halo_copy = pltpu.make_async_remote_copy(
        src_ref=halo_out, dst_ref=halo_in,
        send_sem=halo_send, recv_sem=halo_recv,
        device_id=(lax.rem(me + n - 1, n), core), device_id_type=MESH,
    )
    swap_b = pltpu.make_async_remote_copy(
        src_ref=pk_c, dst_ref=pk_d, send_sem=tp_send.at[1], recv_sem=tp_recv.at[1],
        device_id=(me, other_core), device_id_type=MESH,
    )
    step = 64
    steps = rows // step

    def tap_step(c, r):
        at = pl.ds(r, step)
        cols = pl.ds(pl.multiple_of(c * LANES, LANES), LANES)
        sig = jax.nn.sigmoid(cg[at, cols].astype(F32))
        gated = (cv[at, cols].astype(F32) * sig).astype(BF16).astype(F32)
        for j in range(ntaps):
            h = hgx[c, pl.ds(r + reach - j, step), :]
            tapacc[c, j] = tapacc[c, j] + jnp.sum((gated * h).reshape(step // 8, 8, LANES), axis=0)

    def taps_body(i, carry):
        tap_step(i // (steps - 1), pl.multiple_of(lax.rem(i, steps - 1) * step, step))
        return carry

    def taps_edge(c, carry):
        tap_step(c, rows - step)
        rowsum = jnp.sum(tapacc[c], axis=1)
        at = pl.ds(pl.multiple_of(c * per, 8), ntaps)
        flat[at, :] = rowsum
        return carry

    def conv_step(c, r):
        at = pl.ds(r, step)
        cols = pl.ds(pl.multiple_of(c * LANES, LANES), LANES)
        sig = jax.nn.sigmoid(cg[at, cols].astype(F32))
        value = cv[at, cols].astype(F32)
        total = jnp.zeros((step // 8, 8, LANES), F32)
        for j in range(ntaps):
            h = hgx[c, pl.ds(r + reach - j, step), :].reshape(step // 8, 8, LANES)
            total = total + tapf[c, j] * h
        total = total.reshape(step, LANES)
        gv[at, cols] = (total * sig).astype(BF16)
        gg[at, cols] = (total * value * sig * (1.0 - sig)).astype(BF16)

    def conv_body(i, carry):
        conv_step(i // (steps - 1), pl.multiple_of(lax.rem(i, steps - 1) * step, step))
        return carry

    def conv_edge(c, carry):
        conv_step(c, rows - step)
        return carry

    def peer_of(i):
        return lax.rem(me + i, n)

    def rows_of(device):
        return pl.ds(pl.multiple_of(device * chunk, chunk), chunk)

    def spread_copy(peer, slot):
        return pltpu.make_async_remote_copy(
            src_ref=narrow.at[rows_of(peer)], dst_ref=parts.at[slot],
            send_sem=a_send, recv_sem=a_recv,
            device_id=(peer, core), device_id_type=MESH,
        )

    def collect_copy(peer, owner):
        return pltpu.make_async_remote_copy(
            src_ref=sent, dst_ref=whole.at[rows_of(owner)],
            send_sem=b_send, recv_sem=b_recv,
            device_id=(peer, core), device_id_type=MESH,
        )

    def loop(body):
        def run(i, carry):
            body(peer_of(i))
            return carry

        lax.fori_loop(1, n, run, 0)

    def add_part(peer):
        mine[...] = mine[...] + parts[peer].astype(F32)

    def all_of(buffer, send_sem, recv_sem):
        return pltpu.make_async_remote_copy(
            src_ref=buffer, dst_ref=buffer, send_sem=send_sem, recv_sem=recv_sem,
            device_id=(me, other_core), device_id_type=MESH,
        )

    all_parts = all_of(parts.at[pl.ds(0, n - 1)], a_send, a_recv)
    all_whole = all_of(whole.at[pl.ds(0, (n - 1) * chunk)], b_send, b_recv)
    all_pieces = all_of(sendbuf.at[:, pl.ds(0, n - 1)], rs_send, rs_recv.at[0, 0])

    taps_total = cblocks * (steps - 1)
    for what, i in plan_of(nbits, pieces, halves):
        if what == "far":
            norm_of(i)
            for p in range(i * halves, (i + 1) * halves):
                far(p)
            if i == 0:
                heard(0)
        elif what == "send":
            stage_copy(i, 0).start()
        elif what == "near":
            for p in range(i * halves, (i + 1) * halves):
                near(p)
        elif what == "act":
            if i == 0:
                loads[2].wait()
                rowacc[...] = jnp.zeros_like(rowacc)
            act(i)
            if i == 0 and nbits > 2:
                heard(1)
        elif what == "grads":
            repeat(0, rows // 32, grads, 4)
            pack(pk_c)
            swap_b.start()
            tapacc[...] = jnp.zeros_like(tapacc)
            loads[7].wait()
            for c in range(cblocks):
                for j in range(ntaps):
                    row = taps_ref[j:j + 1, c * LANES:(c + 1) * LANES].astype(F32)
                    tapf[c, j] = jnp.broadcast_to(row, (8, LANES))
            flat[...] = jnp.zeros_like(flat)
        elif what == "height":
            swap_b.wait()
            unpack((pk_c[0] + pk_d[0]) / chan_total, st_a)
            unpack((pk_c[1] + pk_d[1]) / chan_total, st_b)
            height(0, 0)
            halo_out[...] = hgx[:, :halo, :].astype(BF16)

            @pl.when(me > 0)
            def _():
                halo_copy.start()

            repeat(1, rows // 32, height, 3)
            loads[3].wait()
            loads[4].wait()
        elif what == "taps":
            lax.fori_loop(taps_total * i // TAP_CUTS, taps_total * (i + 1) // TAP_CUTS, taps_body, 0, unroll=7)
        elif what == "edge":
            @pl.when(me < n - 1)
            def _():
                halo_copy.wait_recv()

            hgx[:, rows:, :] = jnp.where(me < n - 1, halo_in[...].astype(F32), 0.0)
            lax.fori_loop(0, cblocks, taps_edge, 0, unroll=3)
            for c in range(cblocks):
                for j in range(2):
                    flat[c * per + ntaps + j:c * per + ntaps + j + 1, :] = jnp.sum(
                        rowacc[j, :, c * LANES:(c + 1) * LANES], axis=0, keepdims=True
                    )
        elif what == "spread":
            for b in range(2, nbits - 1):
                heard(b)
            narrow[...] = flat[...].astype(BF16)
            loop(lambda peer: spread_copy(peer, me).start())
            mine[...] = flat[rows_of(me), :]
        elif what == "collect":
            all_parts.wait_recv()
            loop(add_part)
            sent[...] = mine[...].astype(BF16)
            loop(lambda peer: collect_copy(peer, me).start())
            whole[rows_of(me), :] = sent[...]
        elif what == "conv":
            lax.fori_loop(taps_total * i // CONV_CUTS, taps_total * (i + 1) // CONV_CUTS, conv_body, 0, unroll=7)
        elif what == "cedge":
            lax.fori_loop(0, cblocks, conv_edge, 0, unroll=3)
        else:
            arrive(what, i)
    all_whole.wait_recv()
    for c in range(cblocks):
        cols = slice(c * LANES, (c + 1) * LANES)
        found = whole[c * per:(c + 1) * per, :].astype(F32)
        taps_out[:, cols] = found[:ntaps, :]
        gain_out[cols] = found[ntaps, :]
        shift_out[cols] = found[ntaps + 1, :]

    all_parts.wait_send()
    all_whole.wait_send()
    all_pieces.wait_send()

    @pl.when(me > 0)
    def _():
        halo_copy.wait_send()


def place(*refs):
    count = (len(refs) - 1) // 2
    sem = refs[-1]
    copies = [
        pltpu.make_async_copy(src, dst, sem.at[i])
        for i, (src, dst) in enumerate(zip(refs[:count], refs[count:-1]))
    ]
    for copy in copies:
        copy.start()
    for copy in copies:
        copy.wait()


def local(conv_value, conv_gate, conv_out, conv_taps, norm_gain, norm_shift, proj_weight, out_grad):
    rows, chan = conv_value.shape
    ntaps = conv_taps.shape[0]
    width = out_grad.shape[1]
    n = lax.axis_size("sp")
    nbits = n.bit_length() - 1
    assert 1 << nbits == n and lax.axis_size("tp") == 2
    groups = 3
    gcols = chan // groups
    block = width // n
    halves = min(HALVES, block // 8)
    pieces = groups * halves
    part = block // halves
    cblocks = chan // LANES
    halo = 32
    per = -(-(ntaps + 2) // 8) * 8
    chunk = -(-(-(-per * cblocks // n)) // 16) * 16
    dims = (n, nbits, groups, halves, chan * 2)
    hbm = pl.BlockSpec(memory_space=pl.ANY)
    vmem = pl.BlockSpec(memory_space=pltpu.VMEM)
    dma = pltpu.SemaphoreType.DMA
    results = pl.pallas_call(
        functools.partial(kernel, dims),
        out_shape=(
            pltpu.VMEM((rows, chan), BF16),
            pltpu.VMEM((rows, chan), BF16),
            pltpu.VMEM((ntaps, chan), F32),
            pltpu.VMEM((chan,), F32),
            pltpu.VMEM((chan,), F32),
            pltpu.VMEM((block, chan), F32),
        ),
        in_specs=[hbm] * 8,
        out_specs=(vmem,) * 6,
        scratch_shapes=[
            pltpu.VMEM((rows, chan), BF16),
            pltpu.VMEM((rows, chan), BF16),
            pltpu.VMEM((rows, chan), BF16),
            pltpu.VMEM((ntaps, chan), BF16),
            pltpu.VMEM((chan,), F32),
            pltpu.VMEM((chan,), F32),
            pltpu.VMEM((width, chan), BF16),
            pltpu.VMEM((rows, width), BF16),
            pltpu.VMEM((n, block, rows), BF16),
            pltpu.VMEM((rows, chan), BF16),
            pltpu.VMEM((rows, chan), F32),
            pltpu.VMEM((rows, chan), F32),
            pltpu.VMEM((rows, chan), F32),
            pltpu.VMEM((cblocks, rows + halo, LANES), F32),
            pltpu.VMEM((cblocks, halo, LANES), BF16),
            pltpu.VMEM((cblocks, halo, LANES), BF16),
            pltpu.VMEM((rows, LANES), F32),
            pltpu.VMEM((rows, LANES), F32),
            pltpu.VMEM((rows, LANES), F32),
            *[pltpu.VMEM((2, rows // LANES, LANES), F32)] * 4,
            pltpu.VMEM((cblocks, ntaps, 8, LANES), F32),
            pltpu.VMEM((pieces, n // 2, part, gcols), F32),
            pltpu.VMEM((pieces, n, part, gcols), BF16),
            pltpu.VMEM((pieces, n, part, gcols), BF16),
            pltpu.VMEM((cblocks, ntaps, 8, LANES), F32),
            pltpu.VMEM((2, 8, chan), F32),
            pltpu.VMEM((n * chunk, LANES), F32),
            pltpu.VMEM((n * chunk, LANES), BF16),
            pltpu.VMEM((n, chunk, LANES), BF16),
            pltpu.VMEM((chunk, LANES), F32),
            pltpu.VMEM((chunk, LANES), BF16),
            pltpu.VMEM((n * chunk, LANES), BF16),
            dma((8,)),
            dma((2,)), dma((2,)),
            dma, dma,
            dma, dma((pieces, nbits)),
            dma, dma,
            dma, dma,
            pltpu.SemaphoreType.REGULAR((nbits,)),
        ],
        compiler_params=pltpu.CompilerParams(
            collective_id=0, has_side_effects=True, vmem_limit_bytes=60 * 1024 * 1024
        ),
    )(
        conv_value, conv_gate, conv_out, conv_taps, norm_gain, norm_shift, proj_weight, out_grad,
    )
    return pl.pallas_call(
        place,
        out_shape=tuple(jax.ShapeDtypeStruct(x.shape, x.dtype) for x in results),
        in_specs=[vmem] * len(results),
        out_specs=(hbm,) * len(results),
        scratch_shapes=[dma((len(results),))],
    )(*[pltpu.with_memory_space_constraint(x, pltpu.VMEM) for x in results])


def solution(mesh):
    in_specs = (
        P("sp", "tp"),
        P("sp", "tp"),
        P("sp", "tp"),
        P(None, "tp"),
        P("tp"),
        P("tp"),
        P(None, "tp"),
        P("sp", None),
    )
    out_specs = (P("sp", "tp"), P("sp", "tp"), P(None, "tp"), P("tp"), P("tp"), P("sp", "tp"))
    return jax.shard_map(local, mesh=mesh, in_specs=in_specs, out_specs=out_specs, check_vma=False)
```

```python
import functools

import jax
import jax.numpy as jnp
from jax import lax
from jax.experimental import pallas as pl
from jax.experimental.pallas import tpu as pltpu
from jax.sharding import PartitionSpec as P

norm_eps = 1e-05
MESH = pl.DeviceIdType.MESH
F32 = jnp.float32
BF16 = jnp.bfloat16
LANES = 128
HALVES = 4
UNIT = 256
TAP_CUTS = 6
CONV_CUTS = 6
ORDERS = ('byxa', 'yaxb', 'abyx', 'yxba', 'yxab', 'xyba', 'xbya', 'yabx', 'axyb', 'xayb', 'xayb', 'ybxa')
PLAN = [
    ("far", 0), ("send", 0), ("send", 1), ("send", 2), ("far", 1), ("send", 7), ("send", 6), ("far", 2), ("send", 8),
    ("act", 0), ("send", 5), ("act", 1), ("act", 2), ("send", 10), ("act", 3), ("send", 11), ("grads", 0),
    ("near", 2), ("near", 0), ("near", 1), (1, 0), ("height", 0), (6, 0), ("taps", 0), ("conv", 0), ("send", 9),
    ("taps", 1), ("send", 3), ("taps", 2), ("conv", 1), ("taps", 3), ("send", 4), (0, 0), (2, 0), (7, 0), ("taps", 4),
    (8, 0), ("taps", 5), (11, 0), (10, 0), ("conv", 2), (5, 0), (1, 1), ("conv", 3), ("edge", 0), (3, 0),
    ("spread", 0), (6, 1), (4, 0), (9, 0), (7, 1), (8, 1), (2, 1), ("conv", 4), ("conv", 5), (0, 1), (3, 1),
    ("cedge", 0), (11, 1), (10, 1), (1, 2), (5, 1), (6, 2), (4, 1), (0, 2), (8, 2), (2, 2), ("collect", 0), (7, 2),
    (9, 1), (10, 2), (11, 2), (6, 3), (3, 2), (9, 2), (2, 3), (4, 2), (5, 2), (8, 3), (1, 3), (0, 3), (3, 3), (10, 3),
    (11, 3), (7, 3), (9, 3), (5, 3), (4, 3),
]


def repeat(start, stop, body, unroll):
    assert (stop - start) % unroll == 0

    def step(i, carry):
        for u in range(unroll):
            body(start + i * unroll + u, carry)
        return carry

    lax.fori_loop(0, (stop - start) // unroll, step, 0)


def bit(x, b):
    return lax.rem(x // (1 << b), 2)


def split_bits(nbits):
    cuts = [nbits * i // 4 for i in range(5)]
    return [list(range(cuts[i], cuts[i + 1])) for i in range(4)]


def orders_of(nbits, pieces):
    axes = split_bits(nbits)
    names = {"x": axes[0], "y": axes[1], "a": axes[2], "b": axes[3]}
    return [[b for name in ORDERS[p % len(ORDERS)] for b in names[name]] for p in range(pieces)]


def plan_of(nbits, pieces, halves):
    if nbits == 4 and pieces == len(ORDERS):
        return PLAN
    count = pieces // halves
    plan = []
    for g in range(count):
        plan += [("far", g)] + [("send", p) for p in range(g * halves, (g + 1) * halves)]
    plan += [("act", i) for i in range(4)] + [("grads", 0)]
    plan += [("near", g) for g in range(count)] + [("height", 0)]
    plan += [("taps", i) for i in range(TAP_CUTS)] + [("edge", 0), ("spread", 0)]
    for s in range(nbits):
        plan += [(p, s) for p in range(pieces)]
        if s == 0:
            plan += [("conv", i) for i in range(CONV_CUTS)] + [("cedge", 0)]
        if s == nbits - 2:
            plan += [("collect", 0)]
    return plan


def kernel(
    dims,
    cv_hbm, cg_hbm, co_hbm, taps_hbm, gain_hbm, shift_hbm, w_hbm, og_hbm,
    gv, gg, taps_out, gain_out, shift_out, proj_out,
    cv, cg, co, taps_ref, gain_ref, shift_ref, w, og, ogt, active, normed, dsilu, scaled, hgx, halo_out, halo_in,
    st_a, st_b, st_d, pk_a, pk_b, pk_c, pk_d, tapf, acc, sendbuf, recvbuf, tapacc, rowacc, flat, narrow, parts, mine, sent, whole,
    in_sem, tp_send, tp_recv, halo_send, halo_recv,
    rs_send, rs_recv, a_send, a_recv, b_send, b_recv, seen,
):
    n, nbits, groups, halves, chan_total = dims
    pieces = groups * halves
    rows, chan = co.shape
    width = og.shape[1]
    block = width // n
    part = block // halves
    gcols = chan // groups
    cblocks = chan // LANES
    gblocks = gcols // LANES
    ntaps = taps_ref.shape[0]
    reach = ntaps - 1
    halo = hgx.shape[1] - rows
    chunk = mine.shape[0]
    per = -(-(ntaps + 2) // 8) * 8
    me = lax.axis_index("sp")
    core = lax.axis_index("tp")
    other_core = 1 - core
    orders = orders_of(nbits, pieces)
    mybits = [bit(me, b) for b in range(nbits)]

    def partner(b):
        return me + (1 << b) * (1 - 2 * mybits[b])

    loads = [
        pltpu.make_async_copy(src, dst, in_sem.at[i])
        for i, (src, dst) in enumerate(
            (
                (co_hbm, co), (og_hbm, og), (w_hbm, w), (cg_hbm, cg), (cv_hbm, cv),
                (gain_hbm, gain_ref), (shift_hbm, shift_ref), (taps_hbm, taps_ref),
            )
        )
    ]
    loads[0].start()
    loads[5].start()
    loads[6].start()
    loads[1].start()

    barrier = pltpu.get_barrier_semaphore()

    def greet(device, c):
        pl.semaphore_signal(barrier, inc=1, device_id=(device, c), device_id_type=MESH)

    greet(me, other_core)
    for b in range(nbits):
        greet(partner(b), core)
    odd = mybits[0]
    beside = me - 1 + 2 * odd
    outside = jnp.where(odd == 1, me == n - 1, me == 0)

    @pl.when(jnp.logical_not(outside))
    def _():
        greet(beside, core)

    lane_low = lax.broadcasted_iota(jnp.int32, (1, LANES), 1) < LANES // 2
    nt = rows // LANES
    mid = LANES // 2

    def pack(dst):
        for t in range(nt):
            turned = st_a[t * LANES:(t + 1) * LANES, :].T
            dst[0, t:t + 1, :] = turned[:1, :]
            dst[1, t:t + 1, :] = turned[mid:mid + 1, :]

    def unpack(packed, dst):
        for t in range(nt):
            dst[t * LANES:(t + 1) * LANES, :] = jnp.broadcast_to(packed[t:t + 1, :], (LANES, LANES)).T

    def wide(x, count):
        return jnp.concatenate([x] * count, axis=1)

    loads[0].wait()
    for copy in loads[2:5] + loads[7:]:
        copy.start()

    def stats(i, carry):
        at = pl.ds(pl.multiple_of(i * 64, 64), 64)
        h = co[at, :].astype(F32)
        mean = jnp.sum(h, axis=1, keepdims=True) / chan
        d = h - mean
        m2 = jnp.sum(d * d, axis=1, keepdims=True)
        st_a[at, :] = jnp.where(lane_low, mean, m2)
        return carry

    repeat(0, rows // 64, stats, 8)
    pack(pk_a)
    pl.semaphore_wait(barrier, jnp.where(outside, nbits + 1, nbits + 2))
    swap_a = pltpu.make_async_remote_copy(
        src_ref=pk_a, dst_ref=pk_b, send_sem=tp_send.at[0], recv_sem=tp_recv.at[0],
        device_id=(me, other_core), device_id_type=MESH,
    )
    swap_a.start()

    def tell(b):
        pl.semaphore_signal(seen.at[b], inc=1, device_id=(partner(b), core), device_id_type=MESH)

    def heard(b):
        pl.semaphore_wait(seen.at[b], 1)
        if b + 2 < nbits:
            tell(b + 1)

    tell(0)
    loads[1].wait()
    sub = LANES // block

    def transpose(c, carry):
        t = og[:, pl.ds(pl.multiple_of(c * LANES, LANES), LANES)].T
        for s in range(sub):
            ogt[c * sub + s] = t[s * block:(s + 1) * block, :]
        return carry

    lax.fori_loop(0, width // LANES, transpose, 0, unroll=4)
    loads[5].wait()
    loads[6].wait()
    gain = gain_ref[...].reshape(1, chan)
    shift = shift_ref[...].reshape(1, chan)
    swap_a.wait()
    gap = pk_a[0] - pk_b[0]
    variance = (pk_a[1] + pk_b[1] + gap * gap * (0.5 * chan)) / chan_total
    unpack(0.5 * (pk_a[0] + pk_b[0]), st_b)
    unpack(lax.rsqrt(variance + norm_eps), st_d)

    def norm_of(g):
        cols = slice(g * gcols, (g + 1) * gcols)

        def norm(i, carry):
            at = pl.ds(pl.multiple_of(i * 32, 32), 32)
            z = (co[at, cols].astype(F32) - wide(st_b[at, :], gblocks)) * wide(st_d[at, :], gblocks)
            normed[at, cols] = z
            x = z * gain[:, cols] + shift[:, cols]
            sig = jax.nn.sigmoid(x)
            active[at, cols] = (x * sig).astype(BF16)
            dsilu[at, cols] = sig * (1.0 + x * (1.0 - sig))
            return carry

        repeat(0, rows // 32, norm, 4)

    def stage_copy(p, k):
        count = n >> (k + 1)
        off = n - (n >> k)
        return pltpu.make_async_remote_copy(
            src_ref=sendbuf.at[p, pl.ds(off, count)],
            dst_ref=recvbuf.at[p, pl.ds(off, count)],
            send_sem=rs_send,
            recv_sem=rs_recv.at[p, k],
            device_id=(partner(orders[p][k]), core),
            device_id_type=MESH,
        )

    unit = max(1, min(n // 2, UNIT // part))

    def product(p, start):
        g, h = p // halves, p % halves
        found = []
        for i in range(unit):
            place = start + i
            owner = 0
            for k, b in enumerate(orders[p]):
                flip = place >> (nbits - 1 - k) & 1
                owner = owner + (1 - mybits[b] if flip else mybits[b]) * (1 << b)
            found.append(ogt[owner, h * part:(h + 1) * part, :])
        lhs = jnp.concatenate(found, axis=0)
        out = jnp.dot(lhs, active[:, g * gcols:(g + 1) * gcols], preferred_element_type=F32)
        return out.reshape(unit, part, gcols)

    def far(p):
        for i in range(0, n // 2, unit):
            sendbuf[p, i:i + unit] = product(p, n // 2 + i).astype(BF16)

    def near(p):
        for i in range(0, n // 2, unit):
            acc[p, i:i + unit] = product(p, i)

    def arrive(p, k):
        count = n >> (k + 1)
        off = n - (n >> k)
        stage_copy(p, k).wait_recv()
        if k + 1 < nbits:
            keep = count // 2

            def pass_on(i, carry):
                sendbuf[p, off + count + i] = (
                    acc[p, keep + i] + recvbuf[p, off + keep + i].astype(F32)
                ).astype(BF16)
                return carry

            lax.fori_loop(0, count - keep, pass_on, 0)
            stage_copy(p, k + 1).start()

            def take(i, carry):
                acc[p, i] = acc[p, i] + recvbuf[p, off + i].astype(F32)
                return carry

            lax.fori_loop(0, keep, take, 0)
        else:
            g, h = p // halves, p % halves
            proj_out[h * part:(h + 1) * part, g * gcols:(g + 1) * gcols] = (
                acc[p, 0] + recvbuf[p, off].astype(F32)
            )

    def act(i):
        count = rows // 4
        at = slice(i * count, (i + 1) * count)
        scaled[at, :] = jnp.dot(og[at, :], w[...], preferred_element_type=F32)

    def grads(i, carry):
        at = pl.ds(pl.multiple_of(i * 32, 32), 32)
        z = normed[at, :]
        ng = scaled[at, :] * dsilu[at, :]
        ngz = ng * z
        rowacc[0] = rowacc[0] + jnp.sum(ngz.reshape(4, 8, chan), axis=0)
        rowacc[1] = rowacc[1] + jnp.sum(ng.reshape(4, 8, chan), axis=0)
        s = ng * gain
        scaled[at, :] = s
        total = jnp.sum(s, axis=1, keepdims=True)
        dot = jnp.sum(s * z, axis=1, keepdims=True)
        st_a[at, :] = jnp.where(lane_low, total, dot)
        return carry

    def height(i, carry):
        at = pl.ds(pl.multiple_of(i * 32, 32), 32)
        hg = wide(st_d[at, :], cblocks) * (
            scaled[at, :] - wide(st_a[at, :], cblocks) - normed[at, :] * wide(st_b[at, :], cblocks)
        )
        for c in range(cblocks):
            hgx[c, at, :] = hg[:, c * LANES:(c + 1) * LANES]
        return carry

    halo_copy = pltpu.make_async_remote_copy(
        src_ref=halo_out, dst_ref=halo_in,
        send_sem=halo_send, recv_sem=halo_recv,
        device_id=(lax.rem(me + n - 1, n), core), device_id_type=MESH,
    )
    swap_b = pltpu.make_async_remote_copy(
        src_ref=pk_c, dst_ref=pk_d, send_sem=tp_send.at[1], recv_sem=tp_recv.at[1],
        device_id=(me, other_core), device_id_type=MESH,
    )
    step = 64
    steps = rows // step

    def tap_step(c, r):
        at = pl.ds(r, step)
        cols = pl.ds(pl.multiple_of(c * LANES, LANES), LANES)
        sig = jax.nn.sigmoid(cg[at, cols].astype(F32))
        gated = (cv[at, cols].astype(F32) * sig).astype(BF16).astype(F32)
        for j in range(ntaps):
            h = hgx[c, pl.ds(r + reach - j, step), :]
            tapacc[c, j] = tapacc[c, j] + jnp.sum((gated * h).reshape(step // 8, 8, LANES), axis=0)

    def taps_body(i, carry):
        tap_step(i // (steps - 1), pl.multiple_of(lax.rem(i, steps - 1) * step, step))
        return carry

    def taps_edge(c, carry):
        tap_step(c, rows - step)
        rowsum = jnp.sum(tapacc[c], axis=1)
        at = pl.ds(pl.multiple_of(c * per, 8), ntaps)
        flat[at, :] = rowsum
        return carry

    def conv_step(c, r):
        at = pl.ds(r, step)
        cols = pl.ds(pl.multiple_of(c * LANES, LANES), LANES)
        sig = jax.nn.sigmoid(cg[at, cols].astype(F32))
        value = cv[at, cols].astype(F32)
        total = jnp.zeros((step // 8, 8, LANES), F32)
        for j in range(ntaps):
            h = hgx[c, pl.ds(r + reach - j, step), :].reshape(step // 8, 8, LANES)
            total = total + tapf[c, j] * h
        total = total.reshape(step, LANES)
        gv[at, cols] = (total * sig).astype(BF16)
        gg[at, cols] = (total * value * sig * (1.0 - sig)).astype(BF16)

    def conv_body(i, carry):
        conv_step(i // (steps - 1), pl.multiple_of(lax.rem(i, steps - 1) * step, step))
        return carry

    def conv_edge(c, carry):
        conv_step(c, rows - step)
        return carry

    def peer_of(i):
        return lax.rem(me + i, n)

    def rows_of(device):
        return pl.ds(pl.multiple_of(device * chunk, chunk), chunk)

    def spread_copy(peer, slot):
        return pltpu.make_async_remote_copy(
            src_ref=narrow.at[rows_of(peer)], dst_ref=parts.at[slot],
            send_sem=a_send, recv_sem=a_recv,
            device_id=(peer, core), device_id_type=MESH,
        )

    def collect_copy(peer, owner):
        return pltpu.make_async_remote_copy(
            src_ref=sent, dst_ref=whole.at[rows_of(owner)],
            send_sem=b_send, recv_sem=b_recv,
            device_id=(peer, core), device_id_type=MESH,
        )

    def loop(body):
        def run(i, carry):
            body(peer_of(i))
            return carry

        lax.fori_loop(1, n, run, 0)

    def add_part(peer):
        mine[...] = mine[...] + parts[peer].astype(F32)

    def all_of(buffer, send_sem, recv_sem):
        return pltpu.make_async_remote_copy(
            src_ref=buffer, dst_ref=buffer, send_sem=send_sem, recv_sem=recv_sem,
            device_id=(me, other_core), device_id_type=MESH,
        )

    all_parts = all_of(parts.at[pl.ds(0, n - 1)], a_send, a_recv)
    all_whole = all_of(whole.at[pl.ds(0, (n - 1) * chunk)], b_send, b_recv)
    all_pieces = all_of(sendbuf.at[:, pl.ds(0, n - 1)], rs_send, rs_recv.at[0, 0])

    taps_total = cblocks * (steps - 1)
    for what, i in plan_of(nbits, pieces, halves):
        if what == "far":
            norm_of(i)
            for p in range(i * halves, (i + 1) * halves):
                far(p)
            if i == 0:
                heard(0)
        elif what == "send":
            stage_copy(i, 0).start()
        elif what == "near":
            for p in range(i * halves, (i + 1) * halves):
                near(p)
        elif what == "act":
            if i == 0:
                loads[2].wait()
                rowacc[...] = jnp.zeros_like(rowacc)
            act(i)
            if i == 0 and nbits > 2:
                heard(1)
        elif what == "grads":
            repeat(0, rows // 32, grads, 4)
            pack(pk_c)
            swap_b.start()
            tapacc[...] = jnp.zeros_like(tapacc)
            loads[7].wait()
            for c in range(cblocks):
                for j in range(ntaps):
                    row = taps_ref[j:j + 1, c * LANES:(c + 1) * LANES].astype(F32)
                    tapf[c, j] = jnp.broadcast_to(row, (8, LANES))
            flat[...] = jnp.zeros_like(flat)
        elif what == "height":
            swap_b.wait()
            unpack((pk_c[0] + pk_d[0]) / chan_total, st_a)
            unpack((pk_c[1] + pk_d[1]) / chan_total, st_b)
            height(0, 0)
            halo_out[...] = hgx[:, :halo, :].astype(BF16)

            @pl.when(me > 0)
            def _():
                halo_copy.start()

            repeat(1, rows // 32, height, 3)
            loads[3].wait()
            loads[4].wait()
        elif what == "taps":
            lax.fori_loop(taps_total * i // TAP_CUTS, taps_total * (i + 1) // TAP_CUTS, taps_body, 0, unroll=7)
        elif what == "edge":
            @pl.when(me < n - 1)
            def _():
                halo_copy.wait_recv()

            hgx[:, rows:, :] = jnp.where(me < n - 1, halo_in[...].astype(F32), 0.0)
            lax.fori_loop(0, cblocks, taps_edge, 0, unroll=3)
            for c in range(cblocks):
                for j in range(2):
                    flat[c * per + ntaps + j:c * per + ntaps + j + 1, :] = jnp.sum(
                        rowacc[j, :, c * LANES:(c + 1) * LANES], axis=0, keepdims=True
                    )
        elif what == "spread":
            for b in range(2, nbits - 1):
                heard(b)
            narrow[...] = flat[...].astype(BF16)
            loop(lambda peer: spread_copy(peer, me).start())
            mine[...] = flat[rows_of(me), :]
        elif what == "collect":
            all_parts.wait_recv()
            loop(add_part)
            sent[...] = mine[...].astype(BF16)
            loop(lambda peer: collect_copy(peer, me).start())
            whole[rows_of(me), :] = sent[...]
        elif what == "conv":
            lax.fori_loop(taps_total * i // CONV_CUTS, taps_total * (i + 1) // CONV_CUTS, conv_body, 0, unroll=7)
        elif what == "cedge":
            lax.fori_loop(0, cblocks, conv_edge, 0, unroll=3)
        else:
            arrive(what, i)
    all_whole.wait_recv()
    for c in range(cblocks):
        cols = slice(c * LANES, (c + 1) * LANES)
        found = whole[c * per:(c + 1) * per, :].astype(F32)
        taps_out[:, cols] = found[:ntaps, :]
        gain_out[cols] = found[ntaps, :]
        shift_out[cols] = found[ntaps + 1, :]

    all_parts.wait_send()
    all_whole.wait_send()
    all_pieces.wait_send()

    @pl.when(me > 0)
    def _():
        halo_copy.wait_send()


def place(*refs):
    count = (len(refs) - 1) // 2
    sem = refs[-1]
    copies = [
        pltpu.make_async_copy(src, dst, sem.at[i])
        for i, (src, dst) in enumerate(zip(refs[:count], refs[count:-1]))
    ]
    for copy in copies:
        copy.start()
    for copy in copies:
        copy.wait()


def local(conv_value, conv_gate, conv_out, conv_taps, norm_gain, norm_shift, proj_weight, out_grad):
    rows, chan = conv_value.shape
    ntaps = conv_taps.shape[0]
    width = out_grad.shape[1]
    n = lax.axis_size("sp")
    nbits = n.bit_length() - 1
    assert 1 << nbits == n and lax.axis_size("tp") == 2
    groups = 3
    gcols = chan // groups
    block = width // n
    halves = min(HALVES, block // 8)
    pieces = groups * halves
    part = block // halves
    cblocks = chan // LANES
    halo = 32
    per = -(-(ntaps + 2) // 8) * 8
    chunk = -(-(-(-per * cblocks // n)) // 16) * 16
    dims = (n, nbits, groups, halves, chan * 2)
    hbm = pl.BlockSpec(memory_space=pl.ANY)
    vmem = pl.BlockSpec(memory_space=pltpu.VMEM)
    dma = pltpu.SemaphoreType.DMA
    results = pl.pallas_call(
        functools.partial(kernel, dims),
        out_shape=(
            pltpu.VMEM((rows, chan), BF16),
            pltpu.VMEM((rows, chan), BF16),
            pltpu.VMEM((ntaps, chan), F32),
            pltpu.VMEM((chan,), F32),
            pltpu.VMEM((chan,), F32),
            pltpu.VMEM((block, chan), F32),
        ),
        in_specs=[hbm] * 8,
        out_specs=(vmem,) * 6,
        scratch_shapes=[
            pltpu.VMEM((rows, chan), BF16),
            pltpu.VMEM((rows, chan), BF16),
            pltpu.VMEM((rows, chan), BF16),
            pltpu.VMEM((ntaps, chan), BF16),
            pltpu.VMEM((chan,), F32),
            pltpu.VMEM((chan,), F32),
            pltpu.VMEM((width, chan), BF16),
            pltpu.VMEM((rows, width), BF16),
            pltpu.VMEM((n, block, rows), BF16),
            pltpu.VMEM((rows, chan), BF16),
            pltpu.VMEM((rows, chan), F32),
            pltpu.VMEM((rows, chan), F32),
            pltpu.VMEM((rows, chan), F32),
            pltpu.VMEM((cblocks, rows + halo, LANES), F32),
            pltpu.VMEM((cblocks, halo, LANES), BF16),
            pltpu.VMEM((cblocks, halo, LANES), BF16),
            pltpu.VMEM((rows, LANES), F32),
            pltpu.VMEM((rows, LANES), F32),
            pltpu.VMEM((rows, LANES), F32),
            *[pltpu.VMEM((2, rows // LANES, LANES), F32)] * 4,
            pltpu.VMEM((cblocks, ntaps, 8, LANES), F32),
            pltpu.VMEM((pieces, n // 2, part, gcols), F32),
            pltpu.VMEM((pieces, n, part, gcols), BF16),
            pltpu.VMEM((pieces, n, part, gcols), BF16),
            pltpu.VMEM((cblocks, ntaps, 8, LANES), F32),
            pltpu.VMEM((2, 8, chan), F32),
            pltpu.VMEM((n * chunk, LANES), F32),
            pltpu.VMEM((n * chunk, LANES), BF16),
            pltpu.VMEM((n, chunk, LANES), BF16),
            pltpu.VMEM((chunk, LANES), F32),
            pltpu.VMEM((chunk, LANES), BF16),
            pltpu.VMEM((n * chunk, LANES), BF16),
            dma((8,)),
            dma((2,)), dma((2,)),
            dma, dma,
            dma, dma((pieces, nbits)),
            dma, dma,
            dma, dma,
            pltpu.SemaphoreType.REGULAR((nbits,)),
        ],
        compiler_params=pltpu.CompilerParams(
            collective_id=0, has_side_effects=True, vmem_limit_bytes=60 * 1024 * 1024
        ),
    )(
        conv_value, conv_gate, conv_out, conv_taps, norm_gain, norm_shift, proj_weight, out_grad,
    )
    return pl.pallas_call(
        place,
        out_shape=tuple(jax.ShapeDtypeStruct(x.shape, x.dtype) for x in results),
        in_specs=[vmem] * len(results),
        out_specs=(hbm,) * len(results),
        scratch_shapes=[dma((len(results),))],
    )(*[pltpu.with_memory_space_constraint(x, pltpu.VMEM) for x in results])


def solution(mesh):
    in_specs = (
        P("sp", "tp"),
        P("sp", "tp"),
        P("sp", "tp"),
        P(None, "tp"),
        P("tp"),
        P("tp"),
        P(None, "tp"),
        P("sp", None),
    )
    out_specs = (P("sp", "tp"), P("sp", "tp"), P(None, "tp"), P("tp"), P("tp"), P("sp", "tp"))
    return jax.shard_map(local, mesh=mesh, in_specs=in_specs, out_specs=out_specs, check_vma=False)
```
